32 devices in a mesh: sp: 8 (over z, y), tp: 4 (over x, core).
Axes of the slice: x: 2, y: 2, z: 4, core: 2. Of those that a mesh axis runs over, the one named last changes fastest.
Arguments:
- residual_in: bfloat16 [8192, 2048], P(('sp', 'tp')), may hold values from -6 to 6
- queries: bfloat16 [8192, 2048], P('sp', 'tp'), may hold values from -6 to 6
- keys: bfloat16 [8192, 1024], P('sp', 'tp'), may hold values from -6 to 6
- values: bfloat16 [8192, 1024], P('sp', 'tp'), may hold values from -6 to 6
- query_gain: float32 [128], replicated, may hold values from 1 to 7
- key_norm_gain: float32 [128], replicated, may hold values from 1 to 7
- out_weight: bfloat16 [2048, 2048], replicated, may hold values from -0.125 to 0.125
- norm_gain: float32 [2048], replicated, may hold values from 0.1 to 1.9
- up_weight: bfloat16 [2048, 8192], P('sp', 'tp'), may hold values from -0.125 to 0.125
- down_weight: bfloat16 [8192, 2048], P('tp', 'sp'), may hold values from -0.0625 to 0.0625
Outputs:
- residual_out: bfloat16 [8192, 2048], P(('sp', 'tp'))
The draws below stay inside these ranges and needn't reach their ends.
All inputs are finite; a program needn't handle non-finite values.
Results may differ from the reference program's by a relative error of at most 0.017.
The reference program's roundings to bfloat16 on the way count: a program that leaves them out, or rounds other values in their place, can miss the bound.
Values may be sent and summed in bfloat16 or wider, within the bound.
A program may use at most 128 MiB of HBM per device.

```python
import math
import jax
import jax.numpy as jnp
from jax import lax

D = 2048
FF = 8192
QUERY_HEADS = 16
KEY_VALUE_HEADS = 8
HEAD_WIDTH = 128
GRID_W = 64
SEQUENCE_TOKENS = 8192
N_TP = 4


def planted_pair(key):
    key_sample = jnp.clip(jax.random.normal(jax.random.fold_in(key, 11), (SEQUENCE_TOKENS, KEY_VALUE_HEADS * HEAD_WIDTH), jnp.float32), -6.0, 6.0)
    query_draw = jnp.clip(jax.random.normal(jax.random.fold_in(key, 12), (SEQUENCE_TOKENS, QUERY_HEADS * HEAD_WIDTH), jnp.float32), -6.0, 6.0)
    return (query_draw, key_sample)


def draw_queries(key, part):
    return planted_pair(key)[0].astype(jnp.bfloat16)


def draw_keys(key, part):
    return planted_pair(key)[1].astype(jnp.bfloat16)


def gain_draw(key):
    return jnp.clip(3.0 * (1.0 + 0.15 * jax.random.normal(key, (HEAD_WIDTH,), jnp.float32)), 1.0, 7.0)


def draw_query_gain(key, part):
    return gain_draw(jax.random.fold_in(key, 21))


def draw_key_norm_gain(key, part):
    return gain_draw(jax.random.fold_in(key, 22))


def block_scale(own_key, shape, pieces, least, high):
    level = 1.0
    for dim, parts in pieces:
        heights = jax.random.uniform(jax.random.fold_in(jax.random.fold_in(own_key, 6), dim), (parts,), jnp.float32, least / len(pieces), high / len(pieces))
        level = level * jnp.repeat(jnp.exp(heights), shape[dim] // parts).reshape((-1,) + (1,) * (len(shape) - 1 - dim))
    return level


def centred(rng, shape, scale, limit, split=(), held_as=jnp.bfloat16):
    values = jax.random.normal(rng, shape, jnp.float32) * scale
    if len(split) > 0:
        values = block_scale(rng, shape, split, -0.22, 0.18) * values
    return jnp.clip(values, min=-limit, max=limit).astype(held_as)


def setup_inputs(seed: int = 0) -> dict:
    arg_keys = jax.random.split(jax.random.key(seed), 11)
    residual_in = centred(arg_keys[0], (SEQUENCE_TOKENS, D), 1.0, 6.0, ((0, 32),))
    queries = draw_queries(jax.random.fold_in(arg_keys[10], 71), 0)
    keys = draw_keys(jax.random.fold_in(arg_keys[10], 71), 0)
    values = centred(arg_keys[3], (SEQUENCE_TOKENS, KEY_VALUE_HEADS * HEAD_WIDTH), 1.0, 6.0, ((0, 8), (1, 4)))
    query_gain = draw_query_gain(jax.random.fold_in(arg_keys[10], 71), 0)
    key_norm_gain = draw_key_norm_gain(jax.random.fold_in(arg_keys[10], 71), 0)
    out_weight = centred(arg_keys[6], (QUERY_HEADS * HEAD_WIDTH, D), (QUERY_HEADS * HEAD_WIDTH) ** -0.5, 0.125)
    norm_gain = jnp.clip(1.0 + 0.18 * jax.random.normal(arg_keys[7], (D,), jnp.float32), 0.1, 1.9)
    up_weight = centred(arg_keys[8], (D, FF), D ** -0.5, 0.125, ((0, 8), (1, 4)))
    down_weight = centred(arg_keys[9], (FF, D), FF ** -0.5, 0.0625, ((0, 4), (1, 8)))
    return {"residual_in": residual_in, "queries": queries, "keys": keys, "values": values, "query_gain": query_gain, "key_norm_gain": key_norm_gain, "out_weight": out_weight, "norm_gain": norm_gain, "up_weight": up_weight, "down_weight": down_weight}


epsilon = 1e-06

def rope_tables(count):
    places = jnp.arange(count)
    grid_row = (places // GRID_W).astype(jnp.float32)
    grid_col = (places % GRID_W).astype(jnp.float32)
    quarter = HEAD_WIDTH // 4
    inverse = 10000.0 ** (-jnp.arange(quarter, dtype=jnp.float32) / quarter)
    angle_row = grid_row[:, None] * inverse
    angle_col = grid_col[:, None] * inverse
    angles = jnp.concatenate([angle_row, angle_row, angle_col, angle_col], axis=-1)
    return (jnp.cos(angles), jnp.sin(angles))

def normalize_rotate(source, gain, heads, cosine_lookup, sine_lookup):
    count = source.shape[0]
    quarter = HEAD_WIDTH // 4
    vector = source.astype(jnp.float32).reshape(count, heads, HEAD_WIDTH)
    vector = vector * lax.rsqrt(lax.optimization_barrier(jnp.mean(vector * vector, axis=-1, keepdims=True)) + epsilon) * gain
    turned = jnp.concatenate([-vector[..., quarter:2 * quarter], vector[..., :quarter], -vector[..., 3 * quarter:], vector[..., 2 * quarter:3 * quarter]], axis=-1)
    rotated = vector * cosine_lookup[:, None, :] + turned * sine_lookup[:, None, :]
    return rotated.reshape(count, heads * HEAD_WIDTH).astype(jnp.bfloat16)

def reference(residual_in, queries, keys, values, query_gain, key_norm_gain, out_weight, norm_gain, up_weight, down_weight):
    cosine_lookup, sine_lookup = rope_tables(SEQUENCE_TOKENS)
    query_normalize = normalize_rotate(queries, query_gain, QUERY_HEADS, cosine_lookup, sine_lookup)
    key_normalize = normalize_rotate(keys, key_norm_gain, KEY_VALUE_HEADS, cosine_lookup, sine_lookup)
    queries_per_group = QUERY_HEADS // KEY_VALUE_HEADS
    key_lattice = key_normalize.astype(jnp.float32).reshape(SEQUENCE_TOKENS, KEY_VALUE_HEADS, HEAD_WIDTH)
    value_lattice = values.astype(jnp.float32).reshape(SEQUENCE_TOKENS, KEY_VALUE_HEADS, HEAD_WIDTH)
    rows_per_block = math.gcd(SEQUENCE_TOKENS, 256)
    query_tiles = query_normalize.reshape(SEQUENCE_TOKENS // rows_per_block, rows_per_block, KEY_VALUE_HEADS, queries_per_group, HEAD_WIDTH)

    def attend_block(query_block):
        scores = jnp.einsum('tkgd,rkd->tkgr', query_block.astype(jnp.float32), key_lattice) * HEAD_WIDTH ** (-0.5)
        highest = lax.optimization_barrier(jnp.max(scores, axis=-1, keepdims=True))
        weights = jnp.exp(scores - highest)
        denom = lax.optimization_barrier(jnp.sum(weights, axis=-1))
        rounded = lax.optimization_barrier(weights.astype(jnp.bfloat16)).astype(jnp.float32)
        summed = jnp.einsum('tkgr,rkd->tkgd', rounded, value_lattice)
        return (summed / denom[..., None]).astype(jnp.bfloat16)
    attn = lax.map(attend_block, query_tiles).reshape(SEQUENCE_TOKENS, QUERY_HEADS * HEAD_WIDTH)
    middle = residual_in.astype(jnp.float32) + jnp.dot(attn, out_weight, preferred_element_type=jnp.float32)
    normed = (middle * lax.rsqrt(lax.optimization_barrier(jnp.mean(middle * middle, axis=-1, keepdims=True)) + epsilon) * norm_gain).astype(jnp.bfloat16)
    hidden = jax.nn.relu(jnp.dot(normed, up_weight, preferred_element_type=jnp.float32))
    act = (hidden * hidden).astype(jnp.bfloat16)
    width = FF // N_TP
    down = jnp.zeros((SEQUENCE_TOKENS, D), jnp.float32)
    for block_index in range(N_TP):
        partial_sum = jnp.dot(act[:, block_index * width:(block_index + 1) * width], down_weight[block_index * width:(block_index + 1) * width], preferred_element_type=jnp.float32)
        down = down + lax.optimization_barrier(partial_sum.astype(jnp.bfloat16)).astype(jnp.float32)
    return (middle + down).astype(jnp.bfloat16)
```

```python
import functools

import jax
import jax.numpy as jnp
import numpy as np
from jax import lax
from jax.experimental import pallas as pl
from jax.experimental.pallas import tpu as pltpu
from jax.sharding import PartitionSpec as P

HEAD_WIDTH = 128
GRID_W = 64
epsilon = 1e-06
MESH = pl.DeviceIdType.MESH
VALUE, KEY, UP, DOWN = range(4)


def ring_order(mesh):
    count = mesh.shape["sp"]
    width = 0
    try:
        width = len({device.coords[1] for device in mesh.devices.flat})
    except Exception:
        width = 0
    if width < 2 or count % width or (count // width) % 2:
        width = 2
        while width * width < count // 2:
            width *= 2
    depth = count // width
    order = [z * width for z in range(depth)]
    for z in reversed(range(depth)):
        columns = list(range(1, width))
        if (depth - 1 - z) % 2:
            columns.reverse()
        order += [z * width + y for y in columns]
    return order


def lookup(table, index):
    found = jnp.int32(table[0])
    for i, entry in enumerate(table):
        if i:
            found = jnp.where(index == i, jnp.int32(entry), found)
    return found


def rotary_tables(tokens):
    quarter = HEAD_WIDTH // 4
    exponent = -np.arange(quarter, dtype=np.float32) / np.float32(quarter)
    inverse = np.power(np.float64(10000.0), exponent.astype(np.float64)).astype(np.float32)
    sign = np.concatenate([-np.ones(quarter), np.ones(quarter)])

    def parts(count):
        angle = np.arange(count, dtype=np.float32)[:, None] * inverse
        twice = np.concatenate([angle, angle], axis=-1).astype(np.float64)
        return np.cos(twice), np.sin(twice) * sign

    row_cos, row_sin = parts(tokens // GRID_W)
    col_cos, col_sin = parts(GRID_W)
    left = lambda a: jnp.asarray(np.pad(a, ((0, 0), (0, HEAD_WIDTH // 2))).astype(np.float32))
    right = lambda a: jnp.asarray(np.pad(a, ((0, 0), (HEAD_WIDTH // 2, 0))).astype(np.float32))
    return left(row_cos), left(row_sin), right(col_cos), right(col_sin)


def layer_kernel(
    order, tp, residual, queries, keys, values, query_gain, key_gain, row_cos, row_sin, col_cos, col_sin,
    out_weight, norm_gain, up, down, out,
    key_raw, key_own, value_own, up_own, down_own, key_buf, value_buf, up_buf, down_buf, query, attn,
    acc, best, mass, heads, weight, middle, normed, give, take, rest,
    load_sem, ring_send, ring_recv, head_send, head_recv, norm_send, norm_recv, part_send, part_recv,
):
    count = len(order)
    half = count // 2
    me = lax.axis_index("sp")
    rank = lax.axis_index("tp")
    position = {sp: i for i, sp in enumerate(order)}
    at_distance = lambda d: lookup([order[(position[i] + d) % count] for i in range(count)], me)
    target = (at_distance(1), at_distance(-1))
    peer = [rank] + [lookup([i ^ k for i in range(tp)], rank) for k in range(1, tp)]
    far_first = sorted(range(1, tp), key=lambda k: (k < 2, k))

    rows = query.shape[0]
    own_rows = heads.shape[0]
    kv_heads = key_own.shape[1] // HEAD_WIDTH
    q_heads = query.shape[1] // HEAD_WIDTH
    group = q_heads // kv_heads
    tile = min(256, rows)
    scale = HEAD_WIDTH ** (-0.5) * 1.4426950408889634

    loads = [
        pltpu.make_async_copy(src, dst, load_sem.at[i])
        for i, (src, dst) in enumerate((
            (values, value_own), (keys, key_raw), (up, up_own), (queries, attn),
            (down, down_own), (residual, rest), (out_weight, weight),
        ))
    ]
    for load in loads:
        load.start()

    barrier = pltpu.get_barrier_semaphore()
    for device in target:
        pl.semaphore_signal(barrier, inc=1, device_id={"sp": device}, device_id_type=MESH)
    for k in range(1, tp):
        pl.semaphore_signal(barrier, inc=1, device_id={"tp": peer[k]}, device_id_type=MESH)
    pl.semaphore_wait(barrier, 1 + tp)

    rings = ((value_own, value_buf), (key_own, key_buf), (up_own, up_buf), (down_own, down_buf))

    def slot(way, step):
        return (half - 1) * way + step - 1 if step < half else count - 2

    def exists(way, step, part):
        return step < half or (step == half and part == way)

    def ring(kind, way, step, part):
        own, buf = rings[kind]
        size = own.shape[0] // 2
        span = pl.ds(part * size, size)
        return pltpu.make_async_remote_copy(
            src_ref=own.at[span] if step == 1 else buf.at[slot(way, step - 1), span],
            dst_ref=buf.at[slot(way, step), span],
            send_sem=ring_send.at[kind, way, step - 1, part],
            recv_sem=ring_recv.at[kind, way, step - 1, part],
            device_id={"sp": target[way]},
            device_id_type=MESH,
        )

    def launch(kind):
        for part in (0, 1):
            for way in (0, 1):
                ring(kind, way, 1, part).start()

    def relay(kind, step):
        for part in (0, 1):
            for way in (0, 1):
                if exists(way, step, part):
                    ring(kind, way, step, part).wait_recv()
                    if exists(way, step + 1, part):
                        ring(kind, way, step + 1, part).start()

    def rotate(src, gain, dst):
        lane = lax.broadcasted_iota(jnp.int32, (GRID_W, HEAD_WIDTH), 1)
        even = (lane // (HEAD_WIDTH // 4)) % 2 == 0

        def body(r, carry):
            grid_row = me * (rows // GRID_W) + r
            cosine = col_cos[...] + row_cos[pl.ds(grid_row, 1), :]
            sine = col_sin[...] + row_sin[pl.ds(grid_row, 1), :]
            here = pl.ds(pl.multiple_of(r * GRID_W, GRID_W), GRID_W)
            for h in range(src.shape[1] // HEAD_WIDTH):
                cols = pl.ds(h * HEAD_WIDTH, HEAD_WIDTH)
                v = src[here, cols].astype(jnp.float32)
                v = v * lax.rsqrt(jnp.mean(v * v, axis=-1, keepdims=True) + epsilon) * gain[...]
                turned = jnp.where(
                    even,
                    pltpu.roll(v, HEAD_WIDTH - HEAD_WIDTH // 4, 1),
                    pltpu.roll(v, HEAD_WIDTH // 4, 1),
                )
                dst[here, cols] = (v * cosine + turned * sine).astype(dst.dtype)
            return carry

        lax.fori_loop(0, rows // GRID_W, body, 0)

    def flash(key_at, value_at, first):
        def body(index, carry):
            per_head = rows // tile
            kv = index // per_head
            here = pl.ds(pl.multiple_of((index % per_head) * tile, tile), tile)
            kv_cols = pl.ds(pl.multiple_of(kv * HEAD_WIDTH, HEAD_WIDTH), HEAD_WIDTH)
            key = key_at[:, kv_cols]
            value = value_at[:, kv_cols]

            def column(g):
                return pl.ds(pl.multiple_of((kv * group + g) * HEAD_WIDTH, HEAD_WIDTH), HEAD_WIDTH)

            def score(g):
                return lax.dot_general(
                    query[here, column(g)], key, (((1,), (1,)), ((), ())),
                    preferred_element_type=jnp.float32,
                )

            scores = [score(g) for g in range(group)]
            for g in range(group):
                s = scores[g]
                cols = column(g)
                top = jnp.max(s, axis=1, keepdims=True) * scale
                if first:
                    newest = jnp.broadcast_to(top, (tile, HEAD_WIDTH))
                else:
                    old = best[here, cols]
                    newest = jnp.maximum(old, top)
                    factor = jnp.exp2(old - newest)
                p = jnp.exp2(s * scale - newest[:, :1])
                total = jnp.sum(p, axis=1, keepdims=True)
                part = jnp.dot(p.astype(jnp.bfloat16), value, preferred_element_type=jnp.float32)
                best[here, cols] = newest
                if first:
                    mass[here, cols] = jnp.broadcast_to(total, (tile, HEAD_WIDTH))
                    acc[here, cols] = part
                else:
                    mass[here, cols] = mass[here, cols] * factor + total
                    acc[here, cols] = acc[here, cols] * factor + part
            return carry

        lax.fori_loop(0, kv_heads * (rows // tile), body, 0)

    loads[0].wait()
    launch(VALUE)
    loads[1].wait()
    rotate(key_raw, key_gain, key_own)
    launch(KEY)
    loads[2].wait()
    launch(UP)
    loads[3].wait()
    rotate(attn, query_gain, query)
    flash(key_own, value_own, True)
    for step in range(1, half + 1):
        relay(VALUE, step)
        relay(KEY, step)
        if step == half - 1:
            relay(UP, 1)
        for way in (0, 1) if step < half else (0,):
            flash(key_buf.at[slot(way, step)], value_buf.at[slot(way, step)], False)

    width = query.shape[1]
    mine = pl.ds(pl.multiple_of(rank * width, width), width)

    def token_rows(k):
        return pl.ds(pl.multiple_of(peer[k] * own_rows, own_rows), own_rows)

    def head_copy(k):
        return pltpu.make_async_remote_copy(
            src_ref=attn.at[token_rows(k)],
            dst_ref=heads.at[:, mine],
            send_sem=head_send.at[k - 1],
            recv_sem=head_recv.at[k - 1],
            device_id={"tp": peer[k]},
            device_id_type=MESH,
        )

    for k in far_first:
        attn[token_rows(k), :] = (acc[token_rows(k), :] / mass[token_rows(k), :]).astype(attn.dtype)
        head_copy(k).start()
    heads[:, mine] = (acc[token_rows(0), :] / mass[token_rows(0), :]).astype(heads.dtype)

    def head_arrival(k):
        cols = pl.ds(pl.multiple_of(peer[k] * width, width), width)
        return pltpu.make_async_remote_copy(
            src_ref=attn.at[token_rows(k)],
            dst_ref=heads.at[:, cols],
            send_sem=head_send.at[k - 1],
            recv_sem=head_recv.at[k - 1],
            device_id={"tp": peer[k]},
            device_id_type=MESH,
        )

    if half > 2:
        relay(UP, 2)
    for load in loads[4:]:
        load.wait()
    for k in range(1, tp):
        head_arrival(k).wait_recv()

    features = middle.shape[1]
    lanes = min(256, features)

    def feature_cols(c):
        return pl.ds(pl.multiple_of(c * lanes, lanes), lanes)

    def project(c, total):
        cols = feature_cols(c)
        made = rest[:, cols].astype(jnp.float32) + jnp.dot(
            heads[...], weight[:, cols], preferred_element_type=jnp.float32
        )
        middle[:, cols] = made
        return total + jnp.sum(made * made, axis=1, keepdims=True)

    squares = lax.fori_loop(0, features // lanes, project, jnp.zeros((own_rows, 1), jnp.float32))
    inverse = lax.rsqrt(squares / features + epsilon)

    def normalize(c, carry):
        cols = feature_cols(c)
        normed[pl.ds(0, own_rows), cols] = (middle[:, cols] * inverse * norm_gain[:, cols]).astype(normed.dtype)
        return carry

    lax.fori_loop(0, features // lanes, normalize, 0)

    def rows_of(k):
        return pl.ds(k * own_rows, own_rows)

    def norm_copy(k):
        source = 0 if k % 2 == 0 else k - 1
        return pltpu.make_async_remote_copy(
            src_ref=normed.at[rows_of(source)],
            dst_ref=normed.at[rows_of(k)],
            send_sem=norm_send.at[k - 1],
            recv_sem=norm_recv.at[k - 1],
            device_id={"tp": peer[k if k % 2 == 0 else 1]},
            device_id_type=MESH,
        )

    for k in range(2, tp, 2):
        norm_copy(k).start()
    norm_copy(1).start()
    for step in range(3, half):
        relay(UP, step)
    launch(DOWN)
    for k in range(2, tp, 2):
        norm_copy(k).wait_recv()
        norm_copy(k + 1).start()
    for k in range(1, tp, 2):
        norm_copy(k).wait_recv()
    relay(UP, half)

    blocks = [(me, None)]
    for step in range(1, half + 1):
        for way in (0, 1) if step < half else (0,):
            blocks.append((at_distance(step if way else -step), slot(way, step)))

    depth = up_own.shape[0]
    hidden = up_own.shape[1]
    all_rows = tp * own_rows
    row_tile = all_rows // 2
    hid_tile = min(256, hidden)
    act = weight.at[pl.ds(0, all_rows), pl.ds(0, hidden)]

    def units(i, carry):
        here = pl.ds(pl.multiple_of((i % 2) * row_tile, row_tile), row_tile)
        cols = pl.ds(pl.multiple_of((i // 2) * hid_tile, hid_tile), hid_tile)
        total = None
        for source, place in blocks:
            there = pl.ds(pl.multiple_of(source * depth, depth), depth)
            matrix = up_own[:, cols] if place is None else up_buf[place, :, cols]
            product = jnp.dot(normed[here, there], matrix, preferred_element_type=jnp.float32)
            total = product if total is None else total + product
        total = jnp.maximum(total, 0.0)
        act[here, cols] = (total * total).astype(act.dtype)
        return carry

    lax.fori_loop(0, 2 * (hidden // hid_tile), units, 0)

    out_cols = down_own.shape[1]

    def part_copy(c, k):
        return pltpu.make_async_remote_copy(
            src_ref=give.at[c, rows_of(k)],
            dst_ref=take.at[c, rows_of(k - 1)],
            send_sem=part_send.at[c, k - 1],
            recv_sem=part_recv.at[c, k - 1],
            device_id={"tp": peer[k]},
            device_id_type=MESH,
        )

    def contribute(c):
        source, place = blocks[c]
        matrix = down_own[...] if place is None else down_buf[place]
        for low in (row_tile, 0):
            here = pl.ds(low, row_tile)
            give[c, here, :] = jnp.dot(act[here, :], matrix, preferred_element_type=jnp.float32).astype(give.dtype)
            for k in range(1, tp):
                if low <= k * own_rows < low + row_tile:
                    part_copy(c, k).start()
        cols = pl.ds(pl.multiple_of(source * out_cols, out_cols), out_cols)
        middle[:, cols] += give[c, rows_of(0), :].astype(jnp.float32)

    def finish(c):
        source, place = blocks[c]
        cols = pl.ds(pl.multiple_of(source * out_cols, out_cols), out_cols)
        total = middle[:, cols]
        for k in range(1, tp):
            part_copy(c, k).wait_recv()
            total = total + take[c, rows_of(k - 1), :].astype(jnp.float32)
        out[:, cols] = total.astype(out.dtype)

    contribute(0)
    done = 0
    ready = 1
    for step in range(1, half + 1):
        relay(DOWN, step)
        fresh = 2 if step < half else 1
        for c in range(ready, ready + fresh):
            contribute(c)
        for c in range(done, ready):
            finish(c)
        done, ready = ready, ready + fresh
    for c in range(done, ready):
        finish(c)

    for kind in range(4):
        for step in range(1, half + 1):
            for part in (0, 1):
                for way in (0, 1):
                    if exists(way, step, part):
                        ring(kind, way, step, part).wait_send()
    for k in range(1, tp):
        head_copy(k).wait_send()
        norm_copy(k).wait_send()
        for c in range(count):
            part_copy(c, k).wait_send()


def local(
    order, tp, residual_in, queries, keys, values, query_gain, key_norm_gain, out_weight, norm_gain, up_weight, down_weight
):
    count = len(order)
    rows, width = queries.shape
    own_rows, features = residual_in.shape
    tables = rotary_tables(rows * count)
    anywhere = pl.BlockSpec(memory_space=pl.ANY)
    vmem = pl.BlockSpec(memory_space=pltpu.VMEM)
    bf16, f32 = jnp.bfloat16, jnp.float32
    others = lambda a: pltpu.VMEM((count - 1,) + a.shape, bf16)
    dma = pltpu.SemaphoreType.DMA
    return pl.pallas_call(
        functools.partial(layer_kernel, order, tp),
        out_shape=jax.ShapeDtypeStruct(residual_in.shape, bf16),
        in_specs=[anywhere] * 4 + [vmem] * 6 + [anywhere, vmem, anywhere, anywhere],
        out_specs=vmem,
        scratch_shapes=[
            pltpu.VMEM(keys.shape, bf16),
            pltpu.VMEM(keys.shape, bf16),
            pltpu.VMEM(values.shape, bf16),
            pltpu.VMEM(up_weight.shape, bf16),
            pltpu.VMEM(down_weight.shape, bf16),
            others(keys),
            others(values),
            others(up_weight),
            others(down_weight),
            pltpu.VMEM(queries.shape, bf16),
            pltpu.VMEM(queries.shape, bf16),
            pltpu.VMEM(queries.shape, f32),
            pltpu.VMEM(queries.shape, f32),
            pltpu.VMEM(queries.shape, f32),
            pltpu.VMEM((own_rows, width * tp), bf16),
            pltpu.VMEM(out_weight.shape, bf16),
            pltpu.VMEM(residual_in.shape, f32),
            pltpu.VMEM((tp * own_rows, features), bf16),
            pltpu.VMEM((count, tp * own_rows, down_weight.shape[1]), bf16),
            pltpu.VMEM((count, (tp - 1) * own_rows, down_weight.shape[1]), bf16),
            pltpu.VMEM(residual_in.shape, bf16),
            dma((7,)),
            dma((4, 2, count // 2, 2)),
            dma((4, 2, count // 2, 2)),
            dma((tp - 1,)),
            dma((tp - 1,)),
            dma((tp - 1,)),
            dma((tp - 1,)),
            dma((count, tp - 1)),
            dma((count, tp - 1)),
        ],
        compiler_params=pltpu.CompilerParams(
            collective_id=0, has_side_effects=True, vmem_limit_bytes=67043328
        ),
        name="layer",
    )(
        residual_in, queries, keys, values, query_gain[None], key_norm_gain[None], *tables,
        out_weight, norm_gain[None], up_weight, down_weight,
    )


def solution(mesh):
    return jax.shard_map(
        functools.partial(local, ring_order(mesh), mesh.shape["tp"]),
        mesh=mesh,
        in_specs=(
            P(("sp", "tp"), None),
            P("sp", "tp"),
            P("sp", "tp"),
            P("sp", "tp"),
            P(),
            P(),
            P(),
            P(),
            P("sp", "tp"),
            P("tp", "sp"),
        ),
        out_specs=P(("sp", "tp"), None),
        check_vma=False,
    )
```

```python
import functools

import jax
import jax.numpy as jnp
import numpy as np
from jax import lax
from jax.experimental import pallas as pl
from jax.experimental.pallas import tpu as pltpu
from jax.sharding import PartitionSpec as P

HEAD_WIDTH = 128
GRID_W = 64
epsilon = 1e-06
MESH = pl.DeviceIdType.MESH
VALUE, KEY, UP, DOWN = range(4)


def plane_width(mesh):
    count = mesh.shape["sp"]
    width = 0
    try:
        width = len({device.coords[1] for device in mesh.devices.flat})
    except Exception:
        width = 0
    if width < 2 or count % width or (count // width) % 2:
        width = 2
        while width * width < count // 2:
            width *= 2
    return width


def ring_order(mesh):
    count = mesh.shape["sp"]
    width = plane_width(mesh)
    depth = count // width
    order = [z * width for z in range(depth)]
    for z in reversed(range(depth)):
        columns = list(range(1, width))
        if (depth - 1 - z) % 2:
            columns.reverse()
        order += [z * width + y for y in columns]
    return order


def lookup(table, index):
    found = jnp.int32(table[0])
    for i, entry in enumerate(table):
        if i:
            found = jnp.where(index == i, jnp.int32(entry), found)
    return found


def rotary_tables(tokens):
    quarter = HEAD_WIDTH // 4
    exponent = -np.arange(quarter, dtype=np.float32) / np.float32(quarter)
    inverse = np.power(np.float64(10000.0), exponent.astype(np.float64)).astype(np.float32)
    sign = np.concatenate([-np.ones(quarter), np.ones(quarter)])

    def parts(count):
        angle = np.arange(count, dtype=np.float32)[:, None] * inverse
        twice = np.concatenate([angle, angle], axis=-1).astype(np.float64)
        return np.cos(twice), np.sin(twice) * sign

    row_cos, row_sin = parts(tokens // GRID_W)
    col_cos, col_sin = parts(GRID_W)
    left = lambda a: jnp.asarray(np.pad(a, ((0, 0), (0, HEAD_WIDTH // 2))).astype(np.float32))
    right = lambda a: jnp.asarray(np.pad(a, ((0, 0), (HEAD_WIDTH // 2, 0))).astype(np.float32))
    return left(row_cos), left(row_sin), right(col_cos), right(col_sin)


def layer_kernel(
    order, tp, residual, queries, keys, values, query_gain, key_gain, row_cos, row_sin, col_cos, col_sin,
    out_weight, norm_gain, up, down, out,
    key_raw, key_own, value_own, up_own, down_own, key_buf, value_buf, up_buf, down_buf, query, attn,
    acc, best, mass, heads, weight, middle, normed, give, take, rest,
    load_sem, ring_send, ring_recv, head_send, head_recv, norm_send, norm_recv, part_send, part_recv,
):
    count = len(order)
    half = count // 2
    me = lax.axis_index("sp")
    rank = lax.axis_index("tp")
    position = {sp: i for i, sp in enumerate(order)}
    at_distance = lambda d: lookup([order[(position[i] + d) % count] for i in range(count)], me)
    target = (at_distance(1), at_distance(-1))
    peer = [rank] + [lookup([i ^ k for i in range(tp)], rank) for k in range(1, tp)]
    far_first = sorted(range(1, tp), key=lambda k: (k < 2, k))

    rows = query.shape[0]
    own_rows = heads.shape[0]
    kv_heads = key_own.shape[1] // HEAD_WIDTH
    q_heads = query.shape[1] // HEAD_WIDTH
    group = q_heads // kv_heads
    tile = min(256, rows)
    scale = HEAD_WIDTH ** (-0.5) * 1.4426950408889634

    loads = [
        pltpu.make_async_copy(src, dst, load_sem.at[i])
        for i, (src, dst) in enumerate((
            (values, value_own), (keys, key_raw), (up, up_own), (queries, attn),
            (down, down_own), (residual, rest), (out_weight, weight),
        ))
    ]
    for load in loads:
        load.start()

    barrier = pltpu.get_barrier_semaphore()
    for device in target:
        pl.semaphore_signal(barrier, inc=1, device_id={"sp": device}, device_id_type=MESH)
    for k in range(1, tp):
        pl.semaphore_signal(barrier, inc=1, device_id={"tp": peer[k]}, device_id_type=MESH)
    pl.semaphore_wait(barrier, 1 + tp)

    rings = ((value_own, value_buf), (key_own, key_buf), (up_own, up_buf), (down_own, down_buf))

    def slot(way, step):
        return (half - 1) * way + step - 1 if step < half else count - 2

    def exists(way, step, part):
        return step < half or (step == half and part == way)

    def ring(kind, way, step, part):
        own, buf = rings[kind]
        size = own.shape[0] // 2
        span = pl.ds(part * size, size)
        return pltpu.make_async_remote_copy(
            src_ref=own.at[span] if step == 1 else buf.at[slot(way, step - 1), span],
            dst_ref=buf.at[slot(way, step), span],
            send_sem=ring_send.at[kind, way, step - 1, part],
            recv_sem=ring_recv.at[kind, way, step - 1, part],
            device_id={"sp": target[way]},
            device_id_type=MESH,
        )

    def launch(kind):
        for part in (0, 1):
            for way in (0, 1):
                ring(kind, way, 1, part).start()

    def relay(kind, step):
        for part in (0, 1):
            for way in (0, 1):
                if exists(way, step, part):
                    ring(kind, way, step, part).wait_recv()
                    if exists(way, step + 1, part):
                        ring(kind, way, step + 1, part).start()

    def rotate(src, gain, dst):
        lane = lax.broadcasted_iota(jnp.int32, (GRID_W, HEAD_WIDTH), 1)
        even = (lane // (HEAD_WIDTH // 4)) % 2 == 0

        def body(r, carry):
            grid_row = me * (rows // GRID_W) + r
            cosine = col_cos[...] + row_cos[pl.ds(grid_row, 1), :]
            sine = col_sin[...] + row_sin[pl.ds(grid_row, 1), :]
            here = pl.ds(pl.multiple_of(r * GRID_W, GRID_W), GRID_W)
            for h in range(src.shape[1] // HEAD_WIDTH):
                cols = pl.ds(h * HEAD_WIDTH, HEAD_WIDTH)
                v = src[here, cols].astype(jnp.float32)
                v = v * lax.rsqrt(jnp.mean(v * v, axis=-1, keepdims=True) + epsilon) * gain[...]
                turned = jnp.where(
                    even,
                    pltpu.roll(v, HEAD_WIDTH - HEAD_WIDTH // 4, 1),
                    pltpu.roll(v, HEAD_WIDTH // 4, 1),
                )
                dst[here, cols] = (v * cosine + turned * sine).astype(dst.dtype)
            return carry

        lax.fori_loop(0, rows // GRID_W, body, 0)

    def flash(key_at, value_at, first):
        def body(index, carry):
            per_head = rows // tile
            kv = index // per_head
            here = pl.ds(pl.multiple_of((index % per_head) * tile, tile), tile)
            kv_cols = pl.ds(pl.multiple_of(kv * HEAD_WIDTH, HEAD_WIDTH), HEAD_WIDTH)
            key = key_at[:, kv_cols]
            value = value_at[:, kv_cols]

            def column(g):
                return pl.ds(pl.multiple_of((kv * group + g) * HEAD_WIDTH, HEAD_WIDTH), HEAD_WIDTH)

            def score(g):
                return lax.dot_general(
                    query[here, column(g)], key, (((1,), (1,)), ((), ())),
                    preferred_element_type=jnp.float32,
                )

            scores = [score(g) for g in range(group)]
            for g in range(group):
                s = scores[g]
                cols = column(g)
                top = jnp.max(s, axis=1, keepdims=True) * scale
                if first:
                    newest = jnp.broadcast_to(top, (tile, HEAD_WIDTH))
                else:
                    old = best[here, cols]
                    newest = jnp.maximum(old, top)
                    factor = jnp.exp2(old - newest)
                p = jnp.exp2(s * scale - newest[:, :1])
                total = jnp.sum(p, axis=1, keepdims=True)
                part = jnp.dot(p.astype(jnp.bfloat16), value, preferred_element_type=jnp.float32)
                best[here, cols] = newest
                if first:
                    mass[here, cols] = jnp.broadcast_to(total, (tile, HEAD_WIDTH))
                    acc[here, cols] = part
                else:
                    mass[here, cols] = mass[here, cols] * factor + total
                    acc[here, cols] = acc[here, cols] * factor + part
            return carry

        lax.fori_loop(0, kv_heads * (rows // tile), body, 0)

    loads[0].wait()
    launch(VALUE)
    loads[1].wait()
    rotate(key_raw, key_gain, key_own)
    launch(KEY)
    loads[2].wait()
    launch(UP)
    loads[3].wait()
    rotate(attn, query_gain, query)
    flash(key_own, value_own, True)
    for step in range(1, half + 1):
        relay(VALUE, step)
        relay(KEY, step)
        if step == half - 1:
            relay(UP, 1)
        for way in (0, 1) if step < half else (0,):
            flash(key_buf.at[slot(way, step)], value_buf.at[slot(way, step)], False)

    width = query.shape[1]
    mine = pl.ds(pl.multiple_of(rank * width, width), width)

    def token_rows(k):
        return pl.ds(pl.multiple_of(peer[k] * own_rows, own_rows), own_rows)

    def head_copy(k):
        return pltpu.make_async_remote_copy(
            src_ref=attn.at[token_rows(k)],
            dst_ref=heads.at[:, mine],
            send_sem=head_send.at[k - 1],
            recv_sem=head_recv.at[k - 1],
            device_id={"tp": peer[k]},
            device_id_type=MESH,
        )

    for k in far_first:
        attn[token_rows(k), :] = (acc[token_rows(k), :] / mass[token_rows(k), :]).astype(attn.dtype)
        head_copy(k).start()
    heads[:, mine] = (acc[token_rows(0), :] / mass[token_rows(0), :]).astype(heads.dtype)

    def head_arrival(k):
        cols = pl.ds(pl.multiple_of(peer[k] * width, width), width)
        return pltpu.make_async_remote_copy(
            src_ref=attn.at[token_rows(k)],
            dst_ref=heads.at[:, cols],
            send_sem=head_send.at[k - 1],
            recv_sem=head_recv.at[k - 1],
            device_id={"tp": peer[k]},
            device_id_type=MESH,
        )

    if half > 2:
        relay(UP, 2)
    for load in loads[4:]:
        load.wait()
    for k in range(1, tp):
        head_arrival(k).wait_recv()

    features = middle.shape[1]
    lanes = min(256, features)

    def feature_cols(c):
        return pl.ds(pl.multiple_of(c * lanes, lanes), lanes)

    def project(c, total):
        cols = feature_cols(c)
        made = rest[:, cols].astype(jnp.float32) + jnp.dot(
            heads[...], weight[:, cols], preferred_element_type=jnp.float32
        )
        middle[:, cols] = made
        return total + jnp.sum(made * made, axis=1, keepdims=True)

    squares = lax.fori_loop(0, features // lanes, project, jnp.zeros((own_rows, 1), jnp.float32))
    inverse = lax.rsqrt(squares / features + epsilon)

    def normalize(c, carry):
        cols = feature_cols(c)
        normed[pl.ds(0, own_rows), cols] = (middle[:, cols] * inverse * norm_gain[:, cols]).astype(normed.dtype)
        return carry

    lax.fori_loop(0, features // lanes, normalize, 0)

    def rows_of(k):
        return pl.ds(k * own_rows, own_rows)

    def norm_copy(k):
        source = 0 if k % 2 == 0 else k - 1
        return pltpu.make_async_remote_copy(
            src_ref=normed.at[rows_of(source)],
            dst_ref=normed.at[rows_of(k)],
            send_sem=norm_send.at[k - 1],
            recv_sem=norm_recv.at[k - 1],
            device_id={"tp": peer[k if k % 2 == 0 else 1]},
            device_id_type=MESH,
        )

    for k in range(2, tp, 2):
        norm_copy(k).start()
    norm_copy(1).start()
    for step in range(3, half):
        relay(UP, step)
    launch(DOWN)
    for k in range(2, tp, 2):
        norm_copy(k).wait_recv()
        norm_copy(k + 1).start()
    for k in range(1, tp, 2):
        norm_copy(k).wait_recv()
    relay(UP, half)

    blocks = [(me, None)]
    for step in range(1, half + 1):
        for way in (0, 1) if step < half else (0,):
            blocks.append((at_distance(step if way else -step), slot(way, step)))

    depth = up_own.shape[0]
    hidden = up_own.shape[1]
    all_rows = tp * own_rows
    row_tile = all_rows // 2
    hid_tile = min(256, hidden)
    act = weight.at[pl.ds(0, all_rows), pl.ds(0, hidden)]

    def units(i, carry):
        here = pl.ds(pl.multiple_of((i % 2) * row_tile, row_tile), row_tile)
        cols = pl.ds(pl.multiple_of((i // 2) * hid_tile, hid_tile), hid_tile)
        total = None
        for source, place in blocks:
            there = pl.ds(pl.multiple_of(source * depth, depth), depth)
            matrix = up_own[:, cols] if place is None else up_buf[place, :, cols]
            product = jnp.dot(normed[here, there], matrix, preferred_element_type=jnp.float32)
            total = product if total is None else total + product
        total = jnp.maximum(total, 0.0)
        act[here, cols] = (total * total).astype(act.dtype)
        return carry

    lax.fori_loop(0, 2 * (hidden // hid_tile), units, 0)

    out_cols = down_own.shape[1]

    def part_copy(c, k):
        return pltpu.make_async_remote_copy(
            src_ref=give.at[c, rows_of(k)],
            dst_ref=take.at[c, rows_of(k - 1)],
            send_sem=part_send.at[c, k - 1],
            recv_sem=part_recv.at[c, k - 1],
            device_id={"tp": peer[k]},
            device_id_type=MESH,
        )

    def contribute(c):
        source, place = blocks[c]
        matrix = down_own[...] if place is None else down_buf[place]
        for low in (row_tile, 0):
            here = pl.ds(low, row_tile)
            give[c, here, :] = jnp.dot(act[here, :], matrix, preferred_element_type=jnp.float32).astype(give.dtype)
            for k in range(1, tp):
                if low <= k * own_rows < low + row_tile:
                    part_copy(c, k).start()
        cols = pl.ds(pl.multiple_of(source * out_cols, out_cols), out_cols)
        middle[:, cols] += give[c, rows_of(0), :].astype(jnp.float32)

    def finish(c):
        source, place = blocks[c]
        cols = pl.ds(pl.multiple_of(source * out_cols, out_cols), out_cols)
        total = middle[:, cols]
        for k in range(1, tp):
            part_copy(c, k).wait_recv()
            total = total + take[c, rows_of(k - 1), :].astype(jnp.float32)
        out[:, cols] = total.astype(out.dtype)

    contribute(0)
    done = 0
    ready = 1
    for step in range(1, half + 1):
        relay(DOWN, step)
        fresh = 2 if step < half else 1
        for c in range(ready, ready + fresh):
            contribute(c)
        for c in range(done, ready):
            finish(c)
        done, ready = ready, ready + fresh
    for c in range(done, ready):
        finish(c)

    for kind in range(4):
        for step in range(1, half + 1):
            for part in (0, 1):
                for way in (0, 1):
                    if exists(way, step, part):
                        ring(kind, way, step, part).wait_send()
    for k in range(1, tp):
        head_copy(k).wait_send()
        norm_copy(k).wait_send()
        for c in range(count):
            part_copy(c, k).wait_send()


def local(
    order, tp, residual_in, queries, keys, values, query_gain, key_norm_gain, out_weight, norm_gain, up_weight, down_weight
):
    count = len(order)
    rows, width = queries.shape
    own_rows, features = residual_in.shape
    tables = rotary_tables(rows * count)
    anywhere = pl.BlockSpec(memory_space=pl.ANY)
    vmem = pl.BlockSpec(memory_space=pltpu.VMEM)
    bf16, f32 = jnp.bfloat16, jnp.float32
    others = lambda a: pltpu.VMEM((count - 1,) + a.shape, bf16)
    dma = pltpu.SemaphoreType.DMA
    return pl.pallas_call(
        functools.partial(layer_kernel, order, tp),
        out_shape=jax.ShapeDtypeStruct(residual_in.shape, bf16),
        in_specs=[anywhere] * 4 + [vmem] * 6 + [anywhere, vmem, anywhere, anywhere],
        out_specs=vmem,
        scratch_shapes=[
            pltpu.VMEM(keys.shape, bf16),
            pltpu.VMEM(keys.shape, bf16),
            pltpu.VMEM(values.shape, bf16),
            pltpu.VMEM(up_weight.shape, bf16),
            pltpu.VMEM(down_weight.shape, bf16),
            others(keys),
            others(values),
            others(up_weight),
            others(down_weight),
            pltpu.VMEM(queries.shape, bf16),
            pltpu.VMEM(queries.shape, bf16),
            pltpu.VMEM(queries.shape, f32),
            pltpu.VMEM(queries.shape, f32),
            pltpu.VMEM(queries.shape, f32),
            pltpu.VMEM((own_rows, width * tp), bf16),
            pltpu.VMEM(out_weight.shape, bf16),
            pltpu.VMEM(residual_in.shape, f32),
            pltpu.VMEM((tp * own_rows, features), bf16),
            pltpu.VMEM((count, tp * own_rows, down_weight.shape[1]), bf16),
            pltpu.VMEM((count, (tp - 1) * own_rows, down_weight.shape[1]), bf16),
            pltpu.VMEM(residual_in.shape, bf16),
            dma((7,)),
            dma((4, 2, count // 2, 2)),
            dma((4, 2, count // 2, 2)),
            dma((tp - 1,)),
            dma((tp - 1,)),
            dma((tp - 1,)),
            dma((tp - 1,)),
            dma((count, tp - 1)),
            dma((count, tp - 1)),
        ],
        compiler_params=pltpu.CompilerParams(
            collective_id=0, has_side_effects=True, vmem_limit_bytes=67043328
        ),
        name="layer",
    )(
        residual_in, queries, keys, values, query_gain[None], key_norm_gain[None], *tables,
        out_weight, norm_gain[None], up_weight, down_weight,
    )


def paired_kernel(
    depth, tp, residual, queries, keys, values, query_gain, key_gain, row_cos, row_sin, col_cos, col_sin,
    out_weight, norm_gain, up, down, out,
    key_raw, key_spare, key_all, value_all, query_raw, query_spare, query, attn, acc, best, mass, heads,
    weight, middle, normed, up_all, down_all, give, sibling, take, rest,
    load_sem, line_send, line_recv, swap_send, swap_recv, head_send, head_recv, norm_send, norm_recv,
    core_send, core_recv, part_send, part_recv,
):
    me = lax.axis_index("sp")
    rank = lax.axis_index("tp")
    layer = me // 2
    row = me % 2
    mate = me + 1 - 2 * row
    place = (me, mate)
    side = (row, 1 - row)
    peer = [rank] + [lookup([i ^ k for i in range(tp)], rank) for k in range(1, tp)]
    pairs = [(j, k) for k in range(tp) for j in (0, 1) if j or k]
    pairs.sort(key=lambda pair: (pair[1] < 2, -pair[0]))

    rows, own_width = queries.shape
    own_rows = heads.shape[0]
    wide = query.shape[1]
    group = wide // HEAD_WIDTH
    tile = min(256, rows)
    scale = HEAD_WIDTH ** (-0.5) * 1.4426950408889634
    hidden = up_all.shape[1]
    up_rows = up.shape[0]
    out_cols = down.shape[1]

    def block(index, size):
        return pl.ds(pl.multiple_of(index * size, size), size)

    loads = [
        pltpu.make_async_copy(src, dst, load_sem.at[i])
        for i, (src, dst) in enumerate((
            (values.at[:, block(row, HEAD_WIDTH)], value_all.at[me]),
            (keys, key_raw),
            (queries, query_raw),
            (up.at[:, block(row, hidden)], up_all.at[block(me, up_rows)]),
            (down.at[block(row, hidden)], down_all.at[me]),
            (residual, rest),
            (out_weight, weight),
        ))
    ]
    for load in loads:
        load.start()

    def inside(index):
        return (index >= 0) & (index < depth)

    barrier = pltpu.get_barrier_semaphore()
    for j, k in pairs:
        pl.semaphore_signal(barrier, inc=1, device_id={"sp": place[j], "tp": peer[k]}, device_id_type=MESH)
    for step in (-1, 1):

        @pl.when(inside(layer + step))
        def _():
            pl.semaphore_signal(barrier, inc=1, device_id={"sp": me + 2 * step}, device_id_type=MESH)

    ends = jnp.where(layer > 0, 1, 0) + jnp.where(layer < depth - 1, 1, 0)
    pl.semaphore_wait(barrier, len(pairs) + ends)

    def spot(kind, c):
        if kind == UP:
            return up_all.at[block(c, up_rows)]
        return {VALUE: value_all, KEY: key_all, DOWN: down_all}[kind].at[c]

    def line(kind, way, step, part, sender):
        sign = 2 * way - 1
        line_row = part if kind == DOWN else side[part]
        there = spot(kind, (layer + sign * (step - 1 if sender else step)) * 2 + line_row)
        return pltpu.make_async_remote_copy(
            src_ref=there,
            dst_ref=there,
            send_sem=line_send.at[kind, way, step - 1, part],
            recv_sem=line_recv.at[kind, way, step - 1, part],
            device_id={"sp": me - 2 * sign},
            device_id_type=MESH,
        )

    def sends(way, step):
        sign = 2 * way - 1
        return inside(layer + sign * (step - 1)) & inside(layer - sign)

    def launch(kind, part):
        for way in (0, 1):

            @pl.when(sends(way, 1))
            def _():
                line(kind, way, 1, part, True).start()

    def relay(kind, step, part):
        for way in (0, 1):

            @pl.when(inside(layer + (2 * way - 1) * step))
            def _():
                line(kind, way, step, part, False).wait_recv()

            if step < depth - 1:

                @pl.when(sends(way, step + 1))
                def _():
                    line(kind, way, step + 1, part, True).start()

    QUERY = 4

    def swap(kind, sender):
        source = {
            VALUE: lambda: values.at[:, block(side[1], HEAD_WIDTH)],
            KEY: lambda: key_spare,
            UP: lambda: up.at[:, block(side[1], hidden)],
            DOWN: lambda: down.at[block(side[1], hidden)],
            QUERY: lambda: query_spare,
        }[kind]()
        turn = 0 if sender else 1
        there = query.at[block(side[turn], rows)] if kind == QUERY else spot(kind, place[turn])
        return pltpu.make_async_remote_copy(
            src_ref=source,
            dst_ref=there,
            send_sem=swap_send.at[kind],
            recv_sem=swap_recv.at[kind],
            device_id={"sp": mate},
            device_id_type=MESH,
        )

    def rotate(src, first_col, gain, dst, first_row, count):
        lane = lax.broadcasted_iota(jnp.int32, (GRID_W, HEAD_WIDTH), 1)
        even = (lane // (HEAD_WIDTH // 4)) % 2 == 0

        def body(r, carry):
            grid_row = me * (rows // GRID_W) + r
            cosine = col_cos[...] + row_cos[pl.ds(grid_row, 1), :]
            sine = col_sin[...] + row_sin[pl.ds(grid_row, 1), :]
            here = block(r, GRID_W)
            there = pl.ds(pl.multiple_of(first_row + r * GRID_W, GRID_W), GRID_W)
            for h in range(count):
                cols = pl.ds(pl.multiple_of(first_col + h * HEAD_WIDTH, HEAD_WIDTH), HEAD_WIDTH)
                v = src[here, cols].astype(jnp.float32)
                v = v * lax.rsqrt(jnp.mean(v * v, axis=-1, keepdims=True) + epsilon) * gain[...]
                turned = jnp.where(
                    even,
                    pltpu.roll(v, HEAD_WIDTH - HEAD_WIDTH // 4, 1),
                    pltpu.roll(v, HEAD_WIDTH // 4, 1),
                )
                dst[there, pl.ds(h * HEAD_WIDTH, HEAD_WIDTH)] = (v * cosine + turned * sine).astype(dst.dtype)
            return carry

        lax.fori_loop(0, rows // GRID_W, body, 0)

    def flash(c, first, base, length):
        def body(index, carry):
            here = pl.ds(pl.multiple_of(base + index * tile, tile), tile)
            key = key_all[c]
            value = value_all[c]
            columns = [pl.ds(g * HEAD_WIDTH, HEAD_WIDTH) for g in range(group)]
            scores = [
                lax.dot_general(
                    query[here, cols], key, (((1,), (1,)), ((), ())), preferred_element_type=jnp.float32
                )
                for cols in columns
            ]
            for s, cols in zip(scores, columns):
                top = jnp.max(s, axis=1, keepdims=True) * scale
                if first:
                    newest = jnp.broadcast_to(top, (tile, HEAD_WIDTH))
                else:
                    old = best[here, cols]
                    newest = jnp.maximum(old, top)
                    factor = jnp.exp2(old - newest)
                p = jnp.exp2(s * scale - newest[:, :1])
                total = jnp.sum(p, axis=1, keepdims=True)
                part = jnp.dot(p.astype(jnp.bfloat16), value, preferred_element_type=jnp.float32)
                best[here, cols] = newest
                if first:
                    mass[here, cols] = jnp.broadcast_to(total, (tile, HEAD_WIDTH))
                    acc[here, cols] = part
                else:
                    mass[here, cols] = mass[here, cols] * factor + total
                    acc[here, cols] = acc[here, cols] * factor + part
            return carry

        lax.fori_loop(0, length // tile, body, 0)

    def each_way(step, line_row, work):
        def body(way, carry):
            index = layer + (2 * way - 1) * step

            @pl.when(inside(index))
            def _():
                work(index * 2 + line_row)

            return carry

        lax.fori_loop(0, 2, body, 0)

    def attend(step, part):
        each_way(step, side[part], lambda c: flash(c, False, 0, 2 * rows))

    def relay_pair(step, part):
        relay(VALUE, step, part)
        relay(KEY, step, part)

    swap(VALUE, True).start()
    loads[0].wait()
    launch(VALUE, 0)
    loads[1].wait()
    rotate(key_raw, row * HEAD_WIDTH, key_gain, key_all.at[me], 0, 1)
    launch(KEY, 0)
    rotate(key_raw, side[1] * HEAD_WIDTH, key_gain, key_spare, 0, 1)
    swap(KEY, True).start()
    swap(VALUE, False).wait_recv()
    launch(VALUE, 1)
    loads[2].wait()
    rotate(query_raw, side[1] * wide, query_gain, query_spare, 0, group)
    swap(QUERY, True).start()
    swap(KEY, False).wait_recv()
    launch(KEY, 1)
    swap(UP, True).start()
    loads[3].wait()
    launch(UP, 0)
    rotate(query_raw, row * wide, query_gain, query, row * rows, group)
    flash(me, True, row * rows, rows)
    relay_pair(1, 0)
    flash(mate, False, row * rows, rows)
    swap(QUERY, False).wait_recv()
    flash(me, True, side[1] * rows, rows)
    flash(mate, False, side[1] * rows, rows)
    events = [(step, part) for step in range(1, depth) for part in (0, 1)]
    swap_started = False
    for i, (step, part) in enumerate(events):
        later = events[i + 1] if i + 1 < len(events) else None
        if i and step == depth - 1:
            relay_pair(step, part)
        if later is not None and later[0] < depth - 1:
            relay_pair(*later)
        if (later is None or later[0] == depth - 1) and not swap_started:
            swap_started = True
            swap(UP, False).wait_recv()
            launch(UP, 1)
            relay(UP, 1, 0)
            swap(DOWN, True).start()
        attend(step, part)

    width = own_width

    def token_rows(j, k):
        return block(side[j] * tp + peer[k], own_rows)

    def head_copy(j, k, sender):
        at = (row, rank) if sender else (side[j], peer[k])
        cols = pl.ds(pl.multiple_of(at[1] * width + at[0] * wide, wide), wide)
        index = j * tp + k - 1
        return pltpu.make_async_remote_copy(
            src_ref=attn.at[token_rows(j, k)],
            dst_ref=heads.at[:, cols],
            send_sem=head_send.at[index],
            recv_sem=head_recv.at[index],
            device_id={"sp": place[j], "tp": peer[k]},
            device_id_type=MESH,
        )

    for j, k in pairs:
        here = token_rows(j, k)
        attn[here, :] = (acc[here, :] / mass[here, :]).astype(attn.dtype)
        head_copy(j, k, True).start()
    here = token_rows(0, 0)
    heads[:, pl.ds(pl.multiple_of(rank * width + row * wide, wide), wide)] = (acc[here, :] / mass[here, :]).astype(heads.dtype)
    relay(UP, 1, 1)
    for load in loads[4:]:
        load.wait()
    for j, k in pairs:
        head_copy(j, k, False).wait_recv()

    features = middle.shape[1]
    lanes = min(256, features)

    def project(c, total):
        cols = block(c, lanes)
        made = rest[:, cols].astype(jnp.float32) + jnp.dot(
            heads[...], weight[:, cols], preferred_element_type=jnp.float32
        )
        middle[:, cols] = made
        return total + jnp.sum(made * made, axis=1, keepdims=True)

    squares = lax.fori_loop(0, features // lanes, project, jnp.zeros((own_rows, 1), jnp.float32))
    inverse = lax.rsqrt(squares / features + epsilon)

    def normalize(c, carry):
        cols = block(c, lanes)
        normed[pl.ds(0, own_rows), cols] = (middle[:, cols] * inverse * norm_gain[:, cols]).astype(normed.dtype)
        return carry

    lax.fori_loop(0, features // lanes, normalize, 0)

    def rows_of(j, k):
        return pl.ds((j * tp + k) * own_rows, own_rows)

    def norm_copy(j, k):
        if k % 2:
            source, target = (j, k - 1), (0, 1)
        elif j:
            source, target = (0, k), (1, 0)
        else:
            source, target = (0, 0), (0, k)
        index = j * tp + k - 1
        return pltpu.make_async_remote_copy(
            src_ref=normed.at[rows_of(*source)],
            dst_ref=normed.at[rows_of(j, k)],
            send_sem=norm_send.at[index],
            recv_sem=norm_recv.at[index],
            device_id={"sp": place[target[0]], "tp": peer[target[1]]},
            device_id_type=MESH,
        )

    for k in range(2, tp, 2):
        norm_copy(0, k).start()
    norm_copy(1, 0).start()
    norm_copy(0, 1).start()
    for step in range(2, depth - 1):
        for part in (0, 1):
            relay(UP, step, part)
    swap(DOWN, False).wait_recv()
    launch(DOWN, 0)
    launch(DOWN, 1)
    for k in range(2, tp, 2):
        norm_copy(0, k).wait_recv()
        norm_copy(1, k).start()
        norm_copy(0, k + 1).start()
    norm_copy(1, 0).wait_recv()
    norm_copy(1, 1).start()
    for part in (0, 1):
        relay(UP, depth - 1, part)
    for k in range(1, tp, 2):
        norm_copy(0, k).wait_recv()

    all_rows = 2 * tp * own_rows
    row_tile = min(512, tp * own_rows)
    hid_tile = min(256, hidden)
    act = weight.at[pl.ds(0, all_rows), pl.ds(0, hidden)]

    def units(j):
        tiles = tp * own_rows // row_tile

        def body(i, carry):
            here = pl.ds(pl.multiple_of(j * tp * own_rows + (i % tiles) * row_tile, row_tile), row_tile)
            cols = block(i // tiles, hid_tile)
            total = jnp.dot(normed[here, :], up_all[:, cols], preferred_element_type=jnp.float32)
            total = jnp.maximum(total, 0.0)
            act[here, cols] = (total * total).astype(act.dtype)
            return carry

        lax.fori_loop(0, tiles * (hidden // hid_tile), body, 0)

    units(0)
    relay(DOWN, 1, 0)
    for k in range(2, tp, 2):
        norm_copy(1, k).wait_recv()
        norm_copy(1, k + 1).start()
    for k in range(1, tp, 2):
        norm_copy(1, k).wait_recv()
    units(1)

    far = [(j, k) for j, k in pairs if k % 2 == 0]

    def half_rows(j, k):
        return pl.ds((j * (tp // 2) + k // 2) * own_rows, own_rows)

    def core_copy(c, j, k):
        index = j * (tp // 2) + k // 2
        return pltpu.make_async_remote_copy(
            src_ref=give.at[c, rows_of(j, k)],
            dst_ref=sibling.at[c, half_rows(j, k)],
            send_sem=core_send.at[c, index],
            recv_sem=core_recv.at[c, index],
            device_id={"tp": peer[1]},
            device_id_type=MESH,
        )

    def part_copy(c, j, k):
        index = far.index((j, k))
        return pltpu.make_async_remote_copy(
            src_ref=give.at[c, rows_of(j, k)],
            dst_ref=take.at[c, pl.ds(index * own_rows, own_rows)],
            send_sem=part_send.at[c, index],
            recv_sem=part_recv.at[c, index],
            device_id={"sp": place[j], "tp": peer[k]},
            device_id_type=MESH,
        )

    def contribute(c):
        def body(t, carry):
            here = block(t, row_tile)
            give[c, here, :] = jnp.dot(
                act[here, :], down_all[c], preferred_element_type=jnp.float32
            ).astype(give.dtype)
            return carry

        lax.fori_loop(0, all_rows // row_tile, body, 0)
        for j in (0, 1):
            for k in range(1, tp, 2):
                core_copy(c, j, k).start()

        def both(j, k):
            core_copy(c, j, k + 1).wait_recv()
            mine = give[c, rows_of(j, k), :].astype(jnp.float32)
            return mine + sibling[c, half_rows(j, k), :].astype(jnp.float32)

        for j, k in far:
            give[c, rows_of(j, k), :] = both(j, k).astype(give.dtype)
            part_copy(c, j, k).start()
        middle[:, block(c, out_cols)] += both(0, 0)

    def finish(c):
        cols = block(c, out_cols)
        total = middle[:, cols]
        for index, (j, k) in enumerate(far):
            part_copy(c, j, k).wait_recv()
            total = total + take[c, pl.ds(index * own_rows, own_rows), :].astype(jnp.float32)
        out[:, cols] = total.astype(out.dtype)

    relay(DOWN, 1, 1)
    for part in (0, 1):
        contribute(layer * 2 + part)
    for i, (step, part) in enumerate(events):
        if i == len(events) - 1:
            for r in (0, 1):
                finish(layer * 2 + r)
            for old_step, old_part in events[:-3]:
                each_way(old_step, old_part, finish)
        if i > 1:
            relay(DOWN, step, part)
        each_way(step, part, contribute)
    for step, part in events[-3:]:
        each_way(step, part, finish)

    for kind in range(4):
        for step in range(1, depth):
            for part in (0, 1):
                for way in (0, 1):

                    @pl.when(sends(way, step))
                    def _():
                        line(kind, way, step, part, True).wait_send()

    for kind in range(5):
        swap(kind, True).wait_send()
    for j, k in pairs:
        head_copy(j, k, True).wait_send()
        norm_copy(j, k).wait_send()

    def drain(c, carry):
        for j in (0, 1):
            for k in range(1, tp, 2):
                core_copy(c, j, k).wait_send()
        for j, k in far:
            part_copy(c, j, k).wait_send()
        return carry

    lax.fori_loop(0, 2 * depth, drain, 0)


def paired_local(
    depth, tp, residual_in, queries, keys, values, query_gain, key_norm_gain, out_weight, norm_gain, up_weight, down_weight
):
    count = 2 * depth
    rows, width = queries.shape
    own_rows, features = residual_in.shape
    tables = rotary_tables(rows * count)
    anywhere = pl.BlockSpec(memory_space=pl.ANY)
    vmem = pl.BlockSpec(memory_space=pltpu.VMEM)
    bf16, f32 = jnp.bfloat16, jnp.float32
    dma = pltpu.SemaphoreType.DMA
    wide = width // 2
    hidden = up_weight.shape[1] // 2
    out_cols = down_weight.shape[1]
    group_rows = 2 * tp * own_rows
    far = tp - 1
    return pl.pallas_call(
        functools.partial(paired_kernel, depth, tp),
        out_shape=jax.ShapeDtypeStruct(residual_in.shape, bf16),
        in_specs=[anywhere] * 4 + [vmem] * 6 + [anywhere, vmem, anywhere, anywhere],
        out_specs=vmem,
        scratch_shapes=[
            pltpu.VMEM(keys.shape, bf16),
            pltpu.VMEM((rows, HEAD_WIDTH), bf16),
            pltpu.VMEM((count, rows, HEAD_WIDTH), bf16),
            pltpu.VMEM((count, rows, HEAD_WIDTH), bf16),
            pltpu.VMEM(queries.shape, bf16),
            pltpu.VMEM((rows, wide), bf16),
            pltpu.VMEM((2 * rows, wide), bf16),
            pltpu.VMEM((2 * rows, wide), bf16),
            pltpu.VMEM((2 * rows, wide), f32),
            pltpu.VMEM((2 * rows, wide), f32),
            pltpu.VMEM((2 * rows, wide), f32),
            pltpu.VMEM((own_rows, width * tp), bf16),
            pltpu.VMEM(out_weight.shape, bf16),
            pltpu.VMEM(residual_in.shape, f32),
            pltpu.VMEM((group_rows, features), bf16),
            pltpu.VMEM((features, hidden), bf16),
            pltpu.VMEM((count, hidden, out_cols), bf16),
            pltpu.VMEM((count, group_rows, out_cols), bf16),
            pltpu.VMEM((count, group_rows // 2, out_cols), bf16),
            pltpu.VMEM((count, far * own_rows, out_cols), bf16),
            pltpu.VMEM(residual_in.shape, bf16),
            dma((7,)),
            dma((4, 2, depth - 1, 2)),
            dma((4, 2, depth - 1, 2)),
            dma((5,)),
            dma((5,)),
            dma((2 * tp - 1,)),
            dma((2 * tp - 1,)),
            dma((2 * tp - 1,)),
            dma((2 * tp - 1,)),
            dma((count, tp)),
            dma((count, tp)),
            dma((count, far)),
            dma((count, far)),
        ],
        compiler_params=pltpu.CompilerParams(
            collective_id=0, has_side_effects=True, vmem_limit_bytes=67043328
        ),
        name="layer",
    )(
        residual_in, queries, keys, values, query_gain[None], key_norm_gain[None], *tables,
        out_weight, norm_gain[None], up_weight, down_weight,
    )


def solution(mesh):
    order = ring_order(mesh)
    count, tp = mesh.shape["sp"], mesh.shape["tp"]

    def step(*arrays):
        kv_heads = arrays[2].shape[1] // HEAD_WIDTH
        if plane_width(mesh) == 2 and count >= 6 and tp % 2 == 0 and kv_heads == 2:
            return paired_local(count // 2, tp, *arrays)
        return local(order, tp, *arrays)

    return jax.shard_map(
        step,
        mesh=mesh,
        in_specs=(
            P(("sp", "tp"), None),
            P("sp", "tp"),
            P("sp", "tp"),
            P("sp", "tp"),
            P(),
            P(),
            P(),
            P(),
            P("sp", "tp"),
            P("tp", "sp"),
        ),
        out_specs=P(("sp", "tp"), None),
        check_vma=False,
    )
```

```python
import functools

import jax
import jax.numpy as jnp
import numpy as np
from jax import lax
from jax.experimental import pallas as pl
from jax.experimental.pallas import tpu as pltpu
from jax.sharding import PartitionSpec as P

HEAD_WIDTH = 128
GRID_W = 64
epsilon = 1e-06
MESH = pl.DeviceIdType.MESH
VALUE, KEY, UP, DOWN = range(4)


def plane_width(mesh):
    count = mesh.shape["sp"]
    width = 0
    try:
        width = len({device.coords[1] for device in mesh.devices.flat})
    except Exception:
        width = 0
    if width < 2 or count % width or (count // width) % 2:
        width = 2
        while width * width < count // 2:
            width *= 2
    return width


def ring_order(mesh):
    count = mesh.shape["sp"]
    width = plane_width(mesh)
    depth = count // width
    order = [z * width for z in range(depth)]
    for z in reversed(range(depth)):
        columns = list(range(1, width))
        if (depth - 1 - z) % 2:
            columns.reverse()
        order += [z * width + y for y in columns]
    return order


def lookup(table, index):
    found = jnp.int32(table[0])
    for i, entry in enumerate(table):
        if i:
            found = jnp.where(index == i, jnp.int32(entry), found)
    return found


def rotary_tables(tokens):
    quarter = HEAD_WIDTH // 4
    exponent = -np.arange(quarter, dtype=np.float32) / np.float32(quarter)
    inverse = np.power(np.float64(10000.0), exponent.astype(np.float64)).astype(np.float32)
    sign = np.concatenate([-np.ones(quarter), np.ones(quarter)])

    def parts(count):
        angle = np.arange(count, dtype=np.float32)[:, None] * inverse
        twice = np.concatenate([angle, angle], axis=-1).astype(np.float64)
        return np.cos(twice), np.sin(twice) * sign

    row_cos, row_sin = parts(tokens // GRID_W)
    col_cos, col_sin = parts(GRID_W)
    left = lambda a: jnp.asarray(np.pad(a, ((0, 0), (0, HEAD_WIDTH // 2))).astype(np.float32))
    right = lambda a: jnp.asarray(np.pad(a, ((0, 0), (HEAD_WIDTH // 2, 0))).astype(np.float32))
    return left(row_cos), left(row_sin), right(col_cos), right(col_sin)


def layer_kernel(
    order, tp, residual, queries, keys, values, query_gain, key_gain, row_cos, row_sin, col_cos, col_sin,
    out_weight, norm_gain, up, down, out,
    key_raw, key_own, value_own, up_own, down_own, key_buf, value_buf, up_buf, down_buf, query, attn,
    acc, best, mass, heads, weight, middle, normed, give, take, rest,
    load_sem, ring_send, ring_recv, head_send, head_recv, norm_send, norm_recv, part_send, part_recv,
):
    count = len(order)
    half = count // 2
    me = lax.axis_index("sp")
    rank = lax.axis_index("tp")
    position = {sp: i for i, sp in enumerate(order)}
    at_distance = lambda d: lookup([order[(position[i] + d) % count] for i in range(count)], me)
    target = (at_distance(1), at_distance(-1))
    peer = [rank] + [lookup([i ^ k for i in range(tp)], rank) for k in range(1, tp)]
    far_first = sorted(range(1, tp), key=lambda k: (k < 2, k))

    rows = query.shape[0]
    own_rows = heads.shape[0]
    kv_heads = key_own.shape[1] // HEAD_WIDTH
    q_heads = query.shape[1] // HEAD_WIDTH
    group = q_heads // kv_heads
    tile = min(256, rows)
    scale = HEAD_WIDTH ** (-0.5) * 1.4426950408889634

    loads = [
        pltpu.make_async_copy(src, dst, load_sem.at[i])
        for i, (src, dst) in enumerate((
            (values, value_own), (keys, key_raw), (up, up_own), (queries, attn),
            (down, down_own), (residual, rest), (out_weight, weight),
        ))
    ]
    for load in loads:
        load.start()

    barrier = pltpu.get_barrier_semaphore()
    for device in target:
        pl.semaphore_signal(barrier, inc=1, device_id={"sp": device}, device_id_type=MESH)
    for k in range(1, tp):
        pl.semaphore_signal(barrier, inc=1, device_id={"tp": peer[k]}, device_id_type=MESH)
    pl.semaphore_wait(barrier, 1 + tp)

    rings = ((value_own, value_buf), (key_own, key_buf), (up_own, up_buf), (down_own, down_buf))

    def slot(way, step):
        return (half - 1) * way + step - 1 if step < half else count - 2

    def exists(way, step, part):
        return step < half or (step == half and part == way)

    def ring(kind, way, step, part):
        own, buf = rings[kind]
        size = own.shape[0] // 2
        span = pl.ds(part * size, size)
        return pltpu.make_async_remote_copy(
            src_ref=own.at[span] if step == 1 else buf.at[slot(way, step - 1), span],
            dst_ref=buf.at[slot(way, step), span],
            send_sem=ring_send.at[kind, way, step - 1, part],
            recv_sem=ring_recv.at[kind, way, step - 1, part],
            device_id={"sp": target[way]},
            device_id_type=MESH,
        )

    def launch(kind):
        for part in (0, 1):
            for way in (0, 1):
                ring(kind, way, 1, part).start()

    def relay(kind, step):
        for part in (0, 1):
            for way in (0, 1):
                if exists(way, step, part):
                    ring(kind, way, step, part).wait_recv()
                    if exists(way, step + 1, part):
                        ring(kind, way, step + 1, part).start()

    def rotate(src, gain, dst):
        lane = lax.broadcasted_iota(jnp.int32, (GRID_W, HEAD_WIDTH), 1)
        even = (lane // (HEAD_WIDTH // 4)) % 2 == 0

        def body(r, carry):
            grid_row = me * (rows // GRID_W) + r
            cosine = col_cos[...] + row_cos[pl.ds(grid_row, 1), :]
            sine = col_sin[...] + row_sin[pl.ds(grid_row, 1), :]
            here = pl.ds(pl.multiple_of(r * GRID_W, GRID_W), GRID_W)
            for h in range(src.shape[1] // HEAD_WIDTH):
                cols = pl.ds(h * HEAD_WIDTH, HEAD_WIDTH)
                v = src[here, cols].astype(jnp.float32)
                v = v * lax.rsqrt(jnp.mean(v * v, axis=-1, keepdims=True) + epsilon) * gain[...]
                turned = jnp.where(
                    even,
                    pltpu.roll(v, HEAD_WIDTH - HEAD_WIDTH // 4, 1),
                    pltpu.roll(v, HEAD_WIDTH // 4, 1),
                )
                dst[here, cols] = (v * cosine + turned * sine).astype(dst.dtype)
            return carry

        lax.fori_loop(0, rows // GRID_W, body, 0)

    def flash(key_at, value_at, first):
        def body(index, carry):
            per_head = rows // tile
            kv = index // per_head
            here = pl.ds(pl.multiple_of((index % per_head) * tile, tile), tile)
            kv_cols = pl.ds(pl.multiple_of(kv * HEAD_WIDTH, HEAD_WIDTH), HEAD_WIDTH)
            key = key_at[:, kv_cols]
            value = value_at[:, kv_cols]

            def column(g):
                return pl.ds(pl.multiple_of((kv * group + g) * HEAD_WIDTH, HEAD_WIDTH), HEAD_WIDTH)

            def score(g):
                return lax.dot_general(
                    query[here, column(g)], key, (((1,), (1,)), ((), ())),
                    preferred_element_type=jnp.float32,
                )

            scores = [score(g) for g in range(group)]
            for g in range(group):
                s = scores[g]
                cols = column(g)
                top = jnp.max(s, axis=1, keepdims=True) * scale
                if first:
                    newest = jnp.broadcast_to(top, (tile, HEAD_WIDTH))
                else:
                    old = best[here, cols]
                    newest = jnp.maximum(old, top)
                    factor = jnp.exp2(old - newest)
                p = jnp.exp2(s * scale - newest[:, :1])
                total = jnp.sum(p, axis=1, keepdims=True)
                part = jnp.dot(p.astype(jnp.bfloat16), value, preferred_element_type=jnp.float32)
                best[here, cols] = newest
                if first:
                    mass[here, cols] = jnp.broadcast_to(total, (tile, HEAD_WIDTH))
                    acc[here, cols] = part
                else:
                    mass[here, cols] = mass[here, cols] * factor + total
                    acc[here, cols] = acc[here, cols] * factor + part
            return carry

        lax.fori_loop(0, kv_heads * (rows // tile), body, 0)

    loads[0].wait()
    launch(VALUE)
    loads[1].wait()
    rotate(key_raw, key_gain, key_own)
    launch(KEY)
    loads[2].wait()
    launch(UP)
    loads[3].wait()
    rotate(attn, query_gain, query)
    flash(key_own, value_own, True)
    for step in range(1, half + 1):
        relay(VALUE, step)
        relay(KEY, step)
        if step == half - 1:
            relay(UP, 1)
        for way in (0, 1) if step < half else (0,):
            flash(key_buf.at[slot(way, step)], value_buf.at[slot(way, step)], False)

    width = query.shape[1]
    mine = pl.ds(pl.multiple_of(rank * width, width), width)

    def token_rows(k):
        return pl.ds(pl.multiple_of(peer[k] * own_rows, own_rows), own_rows)

    def head_copy(k):
        return pltpu.make_async_remote_copy(
            src_ref=attn.at[token_rows(k)],
            dst_ref=heads.at[:, mine],
            send_sem=head_send.at[k - 1],
            recv_sem=head_recv.at[k - 1],
            device_id={"tp": peer[k]},
            device_id_type=MESH,
        )

    for k in far_first:
        attn[token_rows(k), :] = (acc[token_rows(k), :] / mass[token_rows(k), :]).astype(attn.dtype)
        head_copy(k).start()
    heads[:, mine] = (acc[token_rows(0), :] / mass[token_rows(0), :]).astype(heads.dtype)

    def head_arrival(k):
        cols = pl.ds(pl.multiple_of(peer[k] * width, width), width)
        return pltpu.make_async_remote_copy(
            src_ref=attn.at[token_rows(k)],
            dst_ref=heads.at[:, cols],
            send_sem=head_send.at[k - 1],
            recv_sem=head_recv.at[k - 1],
            device_id={"tp": peer[k]},
            device_id_type=MESH,
        )

    if half > 2:
        relay(UP, 2)
    for load in loads[4:]:
        load.wait()
    for k in range(1, tp):
        head_arrival(k).wait_recv()

    features = middle.shape[1]
    lanes = min(256, features)

    def feature_cols(c):
        return pl.ds(pl.multiple_of(c * lanes, lanes), lanes)

    def project(c, total):
        cols = feature_cols(c)
        made = rest[:, cols].astype(jnp.float32) + jnp.dot(
            heads[...], weight[:, cols], preferred_element_type=jnp.float32
        )
        middle[:, cols] = made
        return total + jnp.sum(made * made, axis=1, keepdims=True)

    squares = lax.fori_loop(0, features // lanes, project, jnp.zeros((own_rows, 1), jnp.float32))
    inverse = lax.rsqrt(squares / features + epsilon)

    def normalize(c, carry):
        cols = feature_cols(c)
        normed[pl.ds(0, own_rows), cols] = (middle[:, cols] * inverse * norm_gain[:, cols]).astype(normed.dtype)
        return carry

    lax.fori_loop(0, features // lanes, normalize, 0)

    def rows_of(k):
        return pl.ds(k * own_rows, own_rows)

    def norm_copy(k):
        source = 0 if k % 2 == 0 else k - 1
        return pltpu.make_async_remote_copy(
            src_ref=normed.at[rows_of(source)],
            dst_ref=normed.at[rows_of(k)],
            send_sem=norm_send.at[k - 1],
            recv_sem=norm_recv.at[k - 1],
            device_id={"tp": peer[k if k % 2 == 0 else 1]},
            device_id_type=MESH,
        )

    for k in range(2, tp, 2):
        norm_copy(k).start()
    norm_copy(1).start()
    for step in range(3, half):
        relay(UP, step)
    launch(DOWN)
    for k in range(2, tp, 2):
        norm_copy(k).wait_recv()
        norm_copy(k + 1).start()
    for k in range(1, tp, 2):
        norm_copy(k).wait_recv()
    relay(UP, half)

    blocks = [(me, None)]
    for step in range(1, half + 1):
        for way in (0, 1) if step < half else (0,):
            blocks.append((at_distance(step if way else -step), slot(way, step)))

    depth = up_own.shape[0]
    hidden = up_own.shape[1]
    all_rows = tp * own_rows
    row_tile = all_rows // 2
    hid_tile = min(256, hidden)
    act = weight.at[pl.ds(0, all_rows), pl.ds(0, hidden)]

    def units(i, carry):
        here = pl.ds(pl.multiple_of((i % 2) * row_tile, row_tile), row_tile)
        cols = pl.ds(pl.multiple_of((i // 2) * hid_tile, hid_tile), hid_tile)
        total = None
        for source, place in blocks:
            there = pl.ds(pl.multiple_of(source * depth, depth), depth)
            matrix = up_own[:, cols] if place is None else up_buf[place, :, cols]
            product = jnp.dot(normed[here, there], matrix, preferred_element_type=jnp.float32)
            total = product if total is None else total + product
        total = jnp.maximum(total, 0.0)
        act[here, cols] = (total * total).astype(act.dtype)
        return carry

    lax.fori_loop(0, 2 * (hidden // hid_tile), units, 0)

    out_cols = down_own.shape[1]

    def part_copy(c, k):
        return pltpu.make_async_remote_copy(
            src_ref=give.at[c, rows_of(k)],
            dst_ref=take.at[c, rows_of(k - 1)],
            send_sem=part_send.at[c, k - 1],
            recv_sem=part_recv.at[c, k - 1],
            device_id={"tp": peer[k]},
            device_id_type=MESH,
        )

    def contribute(c):
        source, place = blocks[c]
        matrix = down_own[...] if place is None else down_buf[place]
        for low in (row_tile, 0):
            here = pl.ds(low, row_tile)
            give[c, here, :] = jnp.dot(act[here, :], matrix, preferred_element_type=jnp.float32).astype(give.dtype)
            for k in range(1, tp):
                if low <= k * own_rows < low + row_tile:
                    part_copy(c, k).start()
        cols = pl.ds(pl.multiple_of(source * out_cols, out_cols), out_cols)
        middle[:, cols] += give[c, rows_of(0), :].astype(jnp.float32)

    def finish(c):
        source, place = blocks[c]
        cols = pl.ds(pl.multiple_of(source * out_cols, out_cols), out_cols)
        total = middle[:, cols]
        for k in range(1, tp):
            part_copy(c, k).wait_recv()
            total = total + take[c, rows_of(k - 1), :].astype(jnp.float32)
        out[:, cols] = total.astype(out.dtype)

    contribute(0)
    done = 0
    ready = 1
    for step in range(1, half + 1):
        relay(DOWN, step)
        fresh = 2 if step < half else 1
        for c in range(ready, ready + fresh):
            contribute(c)
        for c in range(done, ready):
            finish(c)
        done, ready = ready, ready + fresh
    for c in range(done, ready):
        finish(c)

    for kind in range(4):
        for step in range(1, half + 1):
            for part in (0, 1):
                for way in (0, 1):
                    if exists(way, step, part):
                        ring(kind, way, step, part).wait_send()
    for k in range(1, tp):
        head_copy(k).wait_send()
        norm_copy(k).wait_send()
        for c in range(count):
            part_copy(c, k).wait_send()


def local(
    order, tp, residual_in, queries, keys, values, query_gain, key_norm_gain, out_weight, norm_gain, up_weight, down_weight
):
    count = len(order)
    rows, width = queries.shape
    own_rows, features = residual_in.shape
    tables = rotary_tables(rows * count)
    anywhere = pl.BlockSpec(memory_space=pl.ANY)
    vmem = pl.BlockSpec(memory_space=pltpu.VMEM)
    bf16, f32 = jnp.bfloat16, jnp.float32
    others = lambda a: pltpu.VMEM((count - 1,) + a.shape, bf16)
    dma = pltpu.SemaphoreType.DMA
    return pl.pallas_call(
        functools.partial(layer_kernel, order, tp),
        out_shape=jax.ShapeDtypeStruct(residual_in.shape, bf16),
        in_specs=[anywhere] * 4 + [vmem] * 6 + [anywhere, vmem, anywhere, anywhere],
        out_specs=vmem,
        scratch_shapes=[
            pltpu.VMEM(keys.shape, bf16),
            pltpu.VMEM(keys.shape, bf16),
            pltpu.VMEM(values.shape, bf16),
            pltpu.VMEM(up_weight.shape, bf16),
            pltpu.VMEM(down_weight.shape, bf16),
            others(keys),
            others(values),
            others(up_weight),
            others(down_weight),
            pltpu.VMEM(queries.shape, bf16),
            pltpu.VMEM(queries.shape, bf16),
            pltpu.VMEM(queries.shape, f32),
            pltpu.VMEM(queries.shape, f32),
            pltpu.VMEM(queries.shape, f32),
            pltpu.VMEM((own_rows, width * tp), bf16),
            pltpu.VMEM(out_weight.shape, bf16),
            pltpu.VMEM(residual_in.shape, f32),
            pltpu.VMEM((tp * own_rows, features), bf16),
            pltpu.VMEM((count, tp * own_rows, down_weight.shape[1]), bf16),
            pltpu.VMEM((count, (tp - 1) * own_rows, down_weight.shape[1]), bf16),
            pltpu.VMEM(residual_in.shape, bf16),
            dma((7,)),
            dma((4, 2, count // 2, 2)),
            dma((4, 2, count // 2, 2)),
            dma((tp - 1,)),
            dma((tp - 1,)),
            dma((tp - 1,)),
            dma((tp - 1,)),
            dma((count, tp - 1)),
            dma((count, tp - 1)),
        ],
        compiler_params=pltpu.CompilerParams(
            collective_id=0, has_side_effects=True, vmem_limit_bytes=67043328
        ),
        name="layer",
    )(
        residual_in, queries, keys, values, query_gain[None], key_norm_gain[None], *tables,
        out_weight, norm_gain[None], up_weight, down_weight,
    )


def paired_kernel(
    depth, tp, residual, queries, keys, values, query_gain, key_gain, row_cos, row_sin, col_cos, col_sin,
    out_weight, norm_gain, up, down, out,
    key_raw, key_spare, key_all, value_all, query_raw, query_spare, query, attn, acc, best, mass, heads,
    weight, middle, normed, up_all, down_all, give, sibling, take, rest,
    load_sem, line_send, line_recv, swap_send, swap_recv, head_send, head_recv, norm_send, norm_recv,
    core_send, core_recv, part_send, part_recv,
):
    me = lax.axis_index("sp")
    rank = lax.axis_index("tp")
    layer = me // 2
    row = me % 2
    mate = me + 1 - 2 * row
    place = (me, mate)
    side = (row, 1 - row)
    peer = [rank] + [lookup([i ^ k for i in range(tp)], rank) for k in range(1, tp)]
    pairs = [(j, k) for k in range(tp) for j in (0, 1) if j or k]
    pairs.sort(key=lambda pair: (pair[1] < 2, -pair[0]))

    rows, own_width = queries.shape
    own_rows = heads.shape[0]
    wide = query.shape[1]
    group = wide // HEAD_WIDTH
    tile = min(256, rows)
    scale = HEAD_WIDTH ** (-0.5) * 1.4426950408889634
    hidden = up_all.shape[1]
    up_rows = up.shape[0]
    out_cols = down.shape[1]
    half_cols = out_cols // 2

    def block(index, size):
        return pl.ds(pl.multiple_of(index * size, size), size)

    loads = [
        pltpu.make_async_copy(src, dst, load_sem.at[i])
        for i, (src, dst) in enumerate((
            (values.at[:, block(row, HEAD_WIDTH)], value_all.at[me]),
            (keys, key_raw),
            (queries, query_raw),
            (up.at[:, block(row, hidden)], up_all.at[block(me, up_rows)]),
            (down.at[block(row, hidden)], down_all.at[me]),
            (residual, rest),
            (out_weight, weight),
        ))
    ]
    for load in loads:
        load.start()

    def inside(index):
        return (index >= 0) & (index < depth)

    barrier = pltpu.get_barrier_semaphore()
    for j, k in pairs:
        pl.semaphore_signal(barrier, inc=1, device_id={"sp": place[j], "tp": peer[k]}, device_id_type=MESH)
    for step in (-1, 1):

        @pl.when(inside(layer + step))
        def _():
            pl.semaphore_signal(barrier, inc=1, device_id={"sp": me + 2 * step}, device_id_type=MESH)

    ends = jnp.where(layer > 0, 1, 0) + jnp.where(layer < depth - 1, 1, 0)
    pl.semaphore_wait(barrier, len(pairs) + ends)

    def spot(kind, c):
        if kind == UP:
            return up_all.at[block(c, up_rows)]
        return {VALUE: value_all, KEY: key_all, DOWN: down_all}[kind].at[c]

    def pieces(kind, step, part):
        return (1, 2) if kind == DOWN and step == depth - 1 and part else (part,)

    def line(kind, way, step, part, sender):
        sign = 2 * way - 1
        split = kind == DOWN and step == depth - 1 and part
        line_row = min(part, 1) if kind == DOWN else side[part]
        there = spot(kind, (layer + sign * (step - 1 if sender else step)) * 2 + line_row)
        if split:
            there = there.at[:, pl.ds((part - 1) * half_cols, half_cols)]
        return pltpu.make_async_remote_copy(
            src_ref=there,
            dst_ref=there,
            send_sem=line_send.at[kind, way, step - 1, part],
            recv_sem=line_recv.at[kind, way, step - 1, part],
            device_id={"sp": me - 2 * sign},
            device_id_type=MESH,
        )

    def sends(way, step):
        sign = 2 * way - 1
        return inside(layer + sign * (step - 1)) & inside(layer - sign)

    def launch(kind, part):
        for way in (0, 1):

            @pl.when(sends(way, 1))
            def _():
                line(kind, way, 1, part, True).start()

    def relay(kind, step, part):
        for way in (0, 1):

            @pl.when(inside(layer + (2 * way - 1) * step))
            def _():
                line(kind, way, step, part, False).wait_recv()

            if step < depth - 1:

                @pl.when(sends(way, step + 1))
                def _():
                    for piece in pieces(kind, step + 1, part):
                        line(kind, way, step + 1, piece, True).start()

    QUERY = 4

    def swap(kind, sender):
        source = {
            VALUE: lambda: values.at[:, block(side[1], HEAD_WIDTH)],
            KEY: lambda: key_spare,
            UP: lambda: up.at[:, block(side[1], hidden)],
            DOWN: lambda: down.at[block(side[1], hidden)],
            QUERY: lambda: query_spare,
        }[kind]()
        turn = 0 if sender else 1
        there = query.at[block(side[turn], rows)] if kind == QUERY else spot(kind, place[turn])
        return pltpu.make_async_remote_copy(
            src_ref=source,
            dst_ref=there,
            send_sem=swap_send.at[kind],
            recv_sem=swap_recv.at[kind],
            device_id={"sp": mate},
            device_id_type=MESH,
        )

    def rotate(src, first_col, gain, dst, first_row, count):
        lane = lax.broadcasted_iota(jnp.int32, (GRID_W, HEAD_WIDTH), 1)
        even = (lane // (HEAD_WIDTH // 4)) % 2 == 0

        def body(r, carry):
            grid_row = me * (rows // GRID_W) + r
            cosine = col_cos[...] + row_cos[pl.ds(grid_row, 1), :]
            sine = col_sin[...] + row_sin[pl.ds(grid_row, 1), :]
            here = block(r, GRID_W)
            there = pl.ds(pl.multiple_of(first_row + r * GRID_W, GRID_W), GRID_W)
            for h in range(count):
                cols = pl.ds(pl.multiple_of(first_col + h * HEAD_WIDTH, HEAD_WIDTH), HEAD_WIDTH)
                v = src[here, cols].astype(jnp.float32)
                v = v * lax.rsqrt(jnp.mean(v * v, axis=-1, keepdims=True) + epsilon) * gain[...]
                turned = jnp.where(
                    even,
                    pltpu.roll(v, HEAD_WIDTH - HEAD_WIDTH // 4, 1),
                    pltpu.roll(v, HEAD_WIDTH // 4, 1),
                )
                dst[there, pl.ds(h * HEAD_WIDTH, HEAD_WIDTH)] = (v * cosine + turned * sine).astype(dst.dtype)
            return carry

        lax.fori_loop(0, rows // GRID_W, body, 0)

    def flash(c, first, base, length):
        columns = [pl.ds(g * HEAD_WIDTH, HEAD_WIDTH) for g in range(group)]

        def body(index, carry):
            key = key_all[c]
            value = value_all[c]
            value = jnp.concatenate([value, jnp.ones_like(value)], axis=1)
            chains = []
            for u in range(2):
                here = pl.ds(pl.multiple_of(base + (index * 2 + u) * tile, tile), tile)
                for cols in columns:
                    s = lax.dot_general(
                        query[here, cols], key, (((1,), (1,)), ((), ())), preferred_element_type=jnp.float32
                    )
                    chains.append((here, cols, s))
            for here, cols, s in chains:
                top = jnp.max(s, axis=1, keepdims=True) * scale
                if first:
                    newest = jnp.broadcast_to(top, (tile, HEAD_WIDTH))
                else:
                    old = best[here, cols]
                    newest = jnp.maximum(old, top)
                    factor = jnp.exp2(old - newest)
                p = jnp.exp2(s * scale - newest[:, :1])
                made = jnp.dot(p.astype(jnp.bfloat16), value, preferred_element_type=jnp.float32)
                part, total = made[:, :HEAD_WIDTH], made[:, HEAD_WIDTH:]
                best[here, cols] = newest
                if first:
                    mass[here, cols] = total
                    acc[here, cols] = part
                else:
                    mass[here, cols] = mass[here, cols] * factor + total
                    acc[here, cols] = acc[here, cols] * factor + part
            return carry

        lax.fori_loop(0, length // (tile * 2), body, 0)

    def each_way(step, line_row, work):
        def body(way, carry):
            index = layer + (2 * way - 1) * step

            @pl.when(inside(index))
            def _():
                work(index * 2 + line_row)

            return carry

        lax.fori_loop(0, 2, body, 0)

    def attend(step, part):
        each_way(step, side[part], lambda c: flash(c, False, 0, 2 * rows))

    def relay_pair(step, part):
        relay(VALUE, step, part)
        relay(KEY, step, part)

    swap(VALUE, True).start()
    loads[0].wait()
    launch(VALUE, 0)
    loads[1].wait()
    rotate(key_raw, row * HEAD_WIDTH, key_gain, key_all.at[me], 0, 1)
    launch(KEY, 0)
    rotate(key_raw, side[1] * HEAD_WIDTH, key_gain, key_spare, 0, 1)
    swap(KEY, True).start()
    swap(VALUE, False).wait_recv()
    launch(VALUE, 1)
    loads[2].wait()
    rotate(query_raw, side[1] * wide, query_gain, query_spare, 0, group)
    swap(QUERY, True).start()
    swap(KEY, False).wait_recv()
    launch(KEY, 1)
    swap(UP, True).start()
    loads[3].wait()
    launch(UP, 0)
    rotate(query_raw, row * wide, query_gain, query, row * rows, group)
    flash(me, True, row * rows, rows)
    relay_pair(1, 0)
    flash(mate, False, row * rows, rows)
    swap(QUERY, False).wait_recv()
    flash(me, True, side[1] * rows, rows)
    flash(mate, False, side[1] * rows, rows)
    events = [(step, part) for step in range(1, depth) for part in (0, 1)]
    swap_started = False
    for i, (step, part) in enumerate(events):
        later = events[i + 1] if i + 1 < len(events) else None
        if i and step == depth - 1:
            relay_pair(step, part)
        if later is not None and later[0] < depth - 1:
            relay_pair(*later)
        if (later is None or later[0] == depth - 1) and not swap_started:
            swap_started = True
            swap(UP, False).wait_recv()
            launch(UP, 1)
            relay(UP, 1, 0)
            swap(DOWN, True).start()
        attend(step, part)

    width = own_width

    def token_rows(j, k):
        return block(side[j] * tp + peer[k], own_rows)

    def head_copy(j, k, sender):
        at = (row, rank) if sender else (side[j], peer[k])
        cols = pl.ds(pl.multiple_of(at[1] * width + at[0] * wide, wide), wide)
        index = j * tp + k - 1
        return pltpu.make_async_remote_copy(
            src_ref=attn.at[token_rows(j, k)],
            dst_ref=heads.at[:, cols],
            send_sem=head_send.at[index],
            recv_sem=head_recv.at[index],
            device_id={"sp": place[j], "tp": peer[k]},
            device_id_type=MESH,
        )

    for j, k in pairs:
        here = token_rows(j, k)
        attn[here, :] = (acc[here, :] / mass[here, :]).astype(attn.dtype)
        head_copy(j, k, True).start()
    here = token_rows(0, 0)
    heads[:, pl.ds(pl.multiple_of(rank * width + row * wide, wide), wide)] = (acc[here, :] / mass[here, :]).astype(heads.dtype)
    relay(UP, 1, 1)
    for load in loads[4:]:
        load.wait()
    for j, k in pairs:
        head_copy(j, k, False).wait_recv()

    features = middle.shape[1]
    lanes = min(256, features)

    def project(c, total):
        cols = block(c, lanes)
        made = rest[:, cols].astype(jnp.float32) + jnp.dot(
            heads[...], weight[:, cols], preferred_element_type=jnp.float32
        )
        middle[:, cols] = made
        return total + jnp.sum(made * made, axis=1, keepdims=True)

    squares = lax.fori_loop(0, features // lanes, project, jnp.zeros((own_rows, 1), jnp.float32))
    inverse = lax.rsqrt(squares / features + epsilon)

    def normalize(c, carry):
        cols = block(c, lanes)
        normed[pl.ds(0, own_rows), cols] = (middle[:, cols] * inverse * norm_gain[:, cols]).astype(normed.dtype)
        return carry

    lax.fori_loop(0, features // lanes, normalize, 0)

    def rows_of(j, k):
        return pl.ds((j * tp + k) * own_rows, own_rows)

    half_own = own_rows // 2

    def norm_copy(j, k, h):
        size = own_rows if k % 2 else half_own
        if k % 2:
            source, target = (j, k - 1), (0, 1)
        elif j and k:
            source, target = ((1, 0), (0, k)) if h else ((0, k), (1, 0))
        else:
            source, target = (0, 0), (j, k)
        index = j * tp + k - 1
        return pltpu.make_async_remote_copy(
            src_ref=normed.at[pl.ds((source[0] * tp + source[1]) * own_rows + h * half_own, size)],
            dst_ref=normed.at[pl.ds((j * tp + k) * own_rows + h * half_own, size)],
            send_sem=norm_send.at[index, h],
            recv_sem=norm_recv.at[index, h],
            device_id={"sp": place[target[0]], "tp": peer[target[1]]},
            device_id_type=MESH,
        )

    def norm_halves(k):
        return (0,) if k % 2 else (0, 1)

    for h in (0, 1):
        for k in range(2, tp, 2):
            norm_copy(0, k, h).start()
        norm_copy(1, 0, 1 - h).start()
    norm_copy(0, 1, 0).start()
    for step in range(2, depth - 1):
        for part in (0, 1):
            relay(UP, step, part)
    swap(DOWN, False).wait_recv()
    launch(DOWN, 0)
    launch(DOWN, 1)
    for k in range(2, tp, 2):
        norm_copy(0, k, 0).wait_recv()
        norm_copy(1, k, 0).start()
    norm_copy(1, 0, 1).wait_recv()
    for k in range(2, tp, 2):
        norm_copy(1, k, 1).start()
    for k in range(2, tp, 2):
        norm_copy(0, k, 1).wait_recv()
        norm_copy(0, k + 1, 0).start()
    norm_copy(1, 0, 0).wait_recv()
    norm_copy(1, 1, 0).start()
    for part in (0, 1):
        relay(UP, depth - 1, part)
    for k in range(1, tp, 2):
        norm_copy(0, k, 0).wait_recv()

    all_rows = 2 * tp * own_rows
    row_tile = min(512, tp * own_rows)
    hid_tile = min(256, hidden)
    act = weight.at[pl.ds(0, all_rows), pl.ds(0, hidden)]

    def units(j):
        tiles = tp * own_rows // row_tile

        def body(i, carry):
            here = pl.ds(pl.multiple_of(j * tp * own_rows + (i % tiles) * row_tile, row_tile), row_tile)
            cols = block(i // tiles, hid_tile)
            total = jnp.dot(normed[here, :], up_all[:, cols], preferred_element_type=jnp.float32)
            total = jnp.maximum(total, 0.0)
            act[here, cols] = (total * total).astype(act.dtype)
            return carry

        lax.fori_loop(0, tiles * (hidden // hid_tile), body, 0)

    units(0)
    for k in range(2, tp, 2):
        for h in (0, 1):
            norm_copy(1, k, h).wait_recv()
        norm_copy(1, k + 1, 0).start()
    for k in range(1, tp, 2):
        norm_copy(1, k, 0).wait_recv()
    units(1)

    far = [(j, k) for j, k in pairs if k % 2 == 0]

    pair_rows = 2 * own_rows

    def columns_of(h):
        return pl.ds(h * half_cols, half_cols)

    def core_copy(c, t, h):
        return pltpu.make_async_remote_copy(
            src_ref=give.at[c, pl.ds(pl.multiple_of(t * pair_rows + own_rows, own_rows), own_rows), columns_of(h)],
            dst_ref=sibling.at[c, block(t, own_rows), columns_of(h)],
            send_sem=core_send.at[c, t, h],
            recv_sem=core_recv.at[c, t, h],
            device_id={"tp": peer[1]},
            device_id_type=MESH,
        )

    def part_copy(c, j, k, h):
        index = far.index((j, k))
        return pltpu.make_async_remote_copy(
            src_ref=give.at[c, rows_of(j, k), columns_of(h)],
            dst_ref=take.at[c, pl.ds(index * own_rows, own_rows), columns_of(h)],
            send_sem=part_send.at[c, index, h],
            recv_sem=part_recv.at[c, index, h],
            device_id={"sp": place[j], "tp": peer[k]},
            device_id_type=MESH,
        )

    def contribute(c, halves=(0, 1)):
        span = pl.ds(halves[0] * half_cols, len(halves) * half_cols)

        def body(i, carry):
            t = tp - 1 - i
            here = block(t, pair_rows)
            give[c, here, span] = jnp.dot(
                act[here, :], down_all[c, :, span], preferred_element_type=jnp.float32
            ).astype(give.dtype)
            for h in halves:
                core_copy(c, t, h).start()
            return carry

        lax.fori_loop(0, tp, body, 0)

        def both(j, k, h):
            t = j * (tp // 2) + k // 2
            core_copy(c, t, h).wait_recv()
            mine = give[c, rows_of(j, k), columns_of(h)].astype(jnp.float32)
            return mine + sibling[c, pl.ds(t * own_rows, own_rows), columns_of(h)].astype(jnp.float32)

        for j, k in far:
            for h in halves:
                give[c, rows_of(j, k), columns_of(h)] = both(j, k, h).astype(give.dtype)
                part_copy(c, j, k, h).start()
        for h in halves:
            cols = pl.ds(pl.multiple_of(c * out_cols + h * half_cols, half_cols), half_cols)
            middle[:, cols] += both(0, 0, h)

    def finish(c, halves=(0, 1)):
        for h in halves:
            cols = pl.ds(pl.multiple_of(c * out_cols + h * half_cols, half_cols), half_cols)
            total = middle[:, cols]
            for index, (j, k) in enumerate(far):
                part_copy(c, j, k, h).wait_recv()
                total = total + take[c, pl.ds(index * own_rows, own_rows), columns_of(h)].astype(jnp.float32)
            out[:, cols] = total.astype(out.dtype)

    def line_done(kind, steps):
        for step in steps:
            for part in (0,) + pieces(kind, step, 1):
                for way in (0, 1):

                    @pl.when(sends(way, step))
                    def _():
                        line(kind, way, step, part, True).wait_send()

    def drain(c):
        for h in (0, 1):
            for t in range(tp):
                core_copy(c, t, h).wait_send()
            for j, k in far:
                part_copy(c, j, k, h).wait_send()

    def settle(c):
        finish(c)
        drain(c)

    steps = range(1, depth)
    relay(DOWN, 1, 0)
    for part in (0, 1):
        contribute(layer * 2 + part)
    for i, (step, part) in enumerate(events):
        if step == depth - 1:
            if not part:
                for kind in (VALUE, KEY, UP):
                    line_done(kind, steps)
                for kind in range(5):
                    swap(kind, True).wait_send()
                for j, k in pairs:
                    head_copy(j, k, True).wait_send()
                    for h in norm_halves(k):
                        norm_copy(j, k, h).wait_send()
            else:
                for r in (0, 1):
                    settle(layer * 2 + r)
                for event in events[:-4]:
                    each_way(*event, settle)
        if i:
            relay(DOWN, step, part)
        if step == depth - 1 and part:
            each_way(step, part, functools.partial(contribute, halves=(0,)))
            line_done(DOWN, steps[:-1])
            each_way(*events[-4], settle)
            relay(DOWN, step, 2)
            each_way(step, part, functools.partial(contribute, halves=(1,)))
        else:
            each_way(step, part, contribute)
    for event in events[-3:]:
        each_way(*event, settle)
    line_done(DOWN, steps[-1:])


def paired_local(
    depth, tp, residual_in, queries, keys, values, query_gain, key_norm_gain, out_weight, norm_gain, up_weight, down_weight
):
    count = 2 * depth
    rows, width = queries.shape
    own_rows, features = residual_in.shape
    tables = rotary_tables(rows * count)
    anywhere = pl.BlockSpec(memory_space=pl.ANY)
    vmem = pl.BlockSpec(memory_space=pltpu.VMEM)
    bf16, f32 = jnp.bfloat16, jnp.float32
    dma = pltpu.SemaphoreType.DMA
    wide = width // 2
    hidden = up_weight.shape[1] // 2
    out_cols = down_weight.shape[1]
    group_rows = 2 * tp * own_rows
    far = tp - 1
    made = pl.pallas_call(
        functools.partial(paired_kernel, depth, tp),
        out_shape=jax.ShapeDtypeStruct(residual_in.shape, bf16),
        in_specs=[anywhere] * 4 + [vmem] * 6 + [anywhere, vmem, anywhere, anywhere],
        out_specs=vmem,
        scratch_shapes=[
            pltpu.VMEM(keys.shape, bf16),
            pltpu.VMEM((rows, HEAD_WIDTH), bf16),
            pltpu.VMEM((count, rows, HEAD_WIDTH), bf16),
            pltpu.VMEM((count, rows, HEAD_WIDTH), bf16),
            pltpu.VMEM(queries.shape, bf16),
            pltpu.VMEM((rows, wide), bf16),
            pltpu.VMEM((2 * rows, wide), bf16),
            pltpu.VMEM((2 * rows, wide), bf16),
            pltpu.VMEM((2 * rows, wide), f32),
            pltpu.VMEM((2 * rows, wide), f32),
            pltpu.VMEM((2 * rows, wide), f32),
            pltpu.VMEM((own_rows, width * tp), bf16),
            pltpu.VMEM(out_weight.shape, bf16),
            pltpu.VMEM(residual_in.shape, f32),
            pltpu.VMEM((group_rows, features), bf16),
            pltpu.VMEM((features, hidden), bf16),
            pltpu.VMEM((count, hidden, out_cols), bf16),
            pltpu.VMEM((count, group_rows, out_cols), bf16),
            pltpu.VMEM((count, group_rows // 2, out_cols), bf16),
            pltpu.VMEM((count, far * own_rows, out_cols), bf16),
            pltpu.VMEM(residual_in.shape, bf16),
            dma((7,)),
            dma((4, 2, depth - 1, 3)),
            dma((4, 2, depth - 1, 3)),
            dma((5,)),
            dma((5,)),
            dma((2 * tp - 1,)),
            dma((2 * tp - 1,)),
            dma((2 * tp - 1, 2)),
            dma((2 * tp - 1, 2)),
            dma((count, tp, 2)),
            dma((count, tp, 2)),
            dma((count, far, 2)),
            dma((count, far, 2)),
        ],
        compiler_params=pltpu.CompilerParams(
            collective_id=0, has_side_effects=True, vmem_limit_bytes=67043328
        ),
        name="layer",
    )(
        residual_in, queries, keys, values, query_gain[None], key_norm_gain[None], *tables,
        out_weight, norm_gain[None], up_weight, down_weight,
    )
    return pl.pallas_call(
        hand_over,
        out_shape=jax.ShapeDtypeStruct(made.shape, bf16),
        in_specs=[vmem],
        out_specs=anywhere,
        scratch_shapes=[dma],
        name="hand_over",
    )(made)


def hand_over(made, out, sem):
    copy = pltpu.make_async_copy(made, out, sem)
    copy.start()
    copy.wait()


def solution(mesh):
    order = ring_order(mesh)
    count, tp = mesh.shape["sp"], mesh.shape["tp"]

    def step(*arrays):
        kv_heads = arrays[2].shape[1] // HEAD_WIDTH
        if plane_width(mesh) == 2 and count >= 6 and tp % 2 == 0 and kv_heads == 2:
            return paired_local(count // 2, tp, *arrays)
        return local(order, tp, *arrays)

    return jax.shard_map(
        step,
        mesh=mesh,
        in_specs=(
            P(("sp", "tp"), None),
            P("sp", "tp"),
            P("sp", "tp"),
            P("sp", "tp"),
            P(),
            P(),
            P(),
            P(),
            P("sp", "tp"),
            P("tp", "sp"),
        ),
        out_specs=P(("sp", "tp"), None),
        check_vma=False,
    )
```

```python
import functools

import jax
import jax.numpy as jnp
import numpy as np
from jax import lax
from jax.experimental import pallas as pl
from jax.experimental.pallas import tpu as pltpu
from jax.sharding import PartitionSpec as P

HEAD_WIDTH = 128
GRID_W = 64
epsilon = 1e-06
MESH = pl.DeviceIdType.MESH
VALUE, KEY, UP, DOWN = range(4)


def plane_width(mesh):
    count = mesh.shape["sp"]
    width = 0
    try:
        width = len({device.coords[1] for device in mesh.devices.flat})
    except Exception:
        width = 0
    if width < 2 or count % width or (count // width) % 2:
        width = 2
        while width * width < count // 2:
            width *= 2
    return width


def ring_order(mesh):
    count = mesh.shape["sp"]
    width = plane_width(mesh)
    depth = count // width
    order = [z * width for z in range(depth)]
    for z in reversed(range(depth)):
        columns = list(range(1, width))
        if (depth - 1 - z) % 2:
            columns.reverse()
        order += [z * width + y for y in columns]
    return order


def lookup(table, index):
    found = jnp.int32(table[0])
    for i, entry in enumerate(table):
        if i:
            found = jnp.where(index == i, jnp.int32(entry), found)
    return found


def rotary_tables(tokens):
    quarter = HEAD_WIDTH // 4
    exponent = -np.arange(quarter, dtype=np.float32) / np.float32(quarter)
    inverse = np.power(np.float64(10000.0), exponent.astype(np.float64)).astype(np.float32)
    sign = np.concatenate([-np.ones(quarter), np.ones(quarter)])

    def parts(count):
        angle = np.arange(count, dtype=np.float32)[:, None] * inverse
        twice = np.concatenate([angle, angle], axis=-1).astype(np.float64)
        return np.cos(twice), np.sin(twice) * sign

    row_cos, row_sin = parts(tokens // GRID_W)
    col_cos, col_sin = parts(GRID_W)
    left = lambda a: jnp.asarray(np.pad(a, ((0, 0), (0, HEAD_WIDTH // 2))).astype(np.float32))
    right = lambda a: jnp.asarray(np.pad(a, ((0, 0), (HEAD_WIDTH // 2, 0))).astype(np.float32))
    return left(row_cos), left(row_sin), right(col_cos), right(col_sin)


def layer_kernel(
    order, tp, residual, queries, keys, values, query_gain, key_gain, row_cos, row_sin, col_cos, col_sin,
    out_weight, norm_gain, up, down, out,
    key_raw, key_own, value_own, up_own, down_own, key_buf, value_buf, up_buf, down_buf, query, attn,
    acc, best, mass, heads, weight, middle, normed, give, take, rest,
    load_sem, ring_send, ring_recv, head_send, head_recv, norm_send, norm_recv, part_send, part_recv,
):
    count = len(order)
    half = count // 2
    me = lax.axis_index("sp")
    rank = lax.axis_index("tp")
    position = {sp: i for i, sp in enumerate(order)}
    at_distance = lambda d: lookup([order[(position[i] + d) % count] for i in range(count)], me)
    target = (at_distance(1), at_distance(-1))
    peer = [rank] + [lookup([i ^ k for i in range(tp)], rank) for k in range(1, tp)]
    far_first = sorted(range(1, tp), key=lambda k: (k < 2, k))

    rows = query.shape[0]
    own_rows = heads.shape[0]
    kv_heads = key_own.shape[1] // HEAD_WIDTH
    q_heads = query.shape[1] // HEAD_WIDTH
    group = q_heads // kv_heads
    tile = min(256, rows)
    scale = HEAD_WIDTH ** (-0.5) * 1.4426950408889634

    loads = [
        pltpu.make_async_copy(src, dst, load_sem.at[i])
        for i, (src, dst) in enumerate((
            (values, value_own), (keys, key_raw), (up, up_own), (queries, attn),
            (down, down_own), (residual, rest), (out_weight, weight),
        ))
    ]
    for load in loads:
        load.start()

    barrier = pltpu.get_barrier_semaphore()
    for device in target:
        pl.semaphore_signal(barrier, inc=1, device_id={"sp": device}, device_id_type=MESH)
    for k in range(1, tp):
        pl.semaphore_signal(barrier, inc=1, device_id={"tp": peer[k]}, device_id_type=MESH)
    pl.semaphore_wait(barrier, 1 + tp)

    rings = ((value_own, value_buf), (key_own, key_buf), (up_own, up_buf), (down_own, down_buf))

    def slot(way, step):
        return (half - 1) * way + step - 1 if step < half else count - 2

    def exists(way, step, part):
        return step < half or (step == half and part == way)

    def ring(kind, way, step, part):
        own, buf = rings[kind]
        size = own.shape[0] // 2
        span = pl.ds(part * size, size)
        return pltpu.make_async_remote_copy(
            src_ref=own.at[span] if step == 1 else buf.at[slot(way, step - 1), span],
            dst_ref=buf.at[slot(way, step), span],
            send_sem=ring_send.at[kind, way, step - 1, part],
            recv_sem=ring_recv.at[kind, way, step - 1, part],
            device_id={"sp": target[way]},
            device_id_type=MESH,
        )

    def launch(kind):
        for part in (0, 1):
            for way in (0, 1):
                ring(kind, way, 1, part).start()

    def relay(kind, step):
        for part in (0, 1):
            for way in (0, 1):
                if exists(way, step, part):
                    ring(kind, way, step, part).wait_recv()
                    if exists(way, step + 1, part):
                        ring(kind, way, step + 1, part).start()

    def rotate(src, gain, dst):
        lane = lax.broadcasted_iota(jnp.int32, (GRID_W, HEAD_WIDTH), 1)
        even = (lane // (HEAD_WIDTH // 4)) % 2 == 0

        def body(r, carry):
            grid_row = me * (rows // GRID_W) + r
            cosine = col_cos[...] + row_cos[pl.ds(grid_row, 1), :]
            sine = col_sin[...] + row_sin[pl.ds(grid_row, 1), :]
            here = pl.ds(pl.multiple_of(r * GRID_W, GRID_W), GRID_W)
            for h in range(src.shape[1] // HEAD_WIDTH):
                cols = pl.ds(h * HEAD_WIDTH, HEAD_WIDTH)
                v = src[here, cols].astype(jnp.float32)
                v = v * lax.rsqrt(jnp.mean(v * v, axis=-1, keepdims=True) + epsilon) * gain[...]
                turned = jnp.where(
                    even,
                    pltpu.roll(v, HEAD_WIDTH - HEAD_WIDTH // 4, 1),
                    pltpu.roll(v, HEAD_WIDTH // 4, 1),
                )
                dst[here, cols] = (v * cosine + turned * sine).astype(dst.dtype)
            return carry

        lax.fori_loop(0, rows // GRID_W, body, 0)

    def flash(key_at, value_at, first):
        def body(index, carry):
            per_head = rows // tile
            kv = index // per_head
            here = pl.ds(pl.multiple_of((index % per_head) * tile, tile), tile)
            kv_cols = pl.ds(pl.multiple_of(kv * HEAD_WIDTH, HEAD_WIDTH), HEAD_WIDTH)
            key = key_at[:, kv_cols]
            value = value_at[:, kv_cols]

            def column(g):
                return pl.ds(pl.multiple_of((kv * group + g) * HEAD_WIDTH, HEAD_WIDTH), HEAD_WIDTH)

            def score(g):
                return lax.dot_general(
                    query[here, column(g)], key, (((1,), (1,)), ((), ())),
                    preferred_element_type=jnp.float32,
                )

            scores = [score(g) for g in range(group)]
            for g in range(group):
                s = scores[g]
                cols = column(g)
                top = jnp.max(s, axis=1, keepdims=True) * scale
                if first:
                    newest = jnp.broadcast_to(top, (tile, HEAD_WIDTH))
                else:
                    old = best[here, cols]
                    newest = jnp.maximum(old, top)
                    factor = jnp.exp2(old - newest)
                p = jnp.exp2(s * scale - newest[:, :1])
                total = jnp.sum(p, axis=1, keepdims=True)
                part = jnp.dot(p.astype(jnp.bfloat16), value, preferred_element_type=jnp.float32)
                best[here, cols] = newest
                if first:
                    mass[here, cols] = jnp.broadcast_to(total, (tile, HEAD_WIDTH))
                    acc[here, cols] = part
                else:
                    mass[here, cols] = mass[here, cols] * factor + total
                    acc[here, cols] = acc[here, cols] * factor + part
            return carry

        lax.fori_loop(0, kv_heads * (rows // tile), body, 0)

    loads[0].wait()
    launch(VALUE)
    loads[1].wait()
    rotate(key_raw, key_gain, key_own)
    launch(KEY)
    loads[2].wait()
    launch(UP)
    loads[3].wait()
    rotate(attn, query_gain, query)
    flash(key_own, value_own, True)
    for step in range(1, half + 1):
        relay(VALUE, step)
        relay(KEY, step)
        if step == half - 1:
            relay(UP, 1)
        for way in (0, 1) if step < half else (0,):
            flash(key_buf.at[slot(way, step)], value_buf.at[slot(way, step)], False)

    width = query.shape[1]
    mine = pl.ds(pl.multiple_of(rank * width, width), width)

    def token_rows(k):
        return pl.ds(pl.multiple_of(peer[k] * own_rows, own_rows), own_rows)

    def head_copy(k):
        return pltpu.make_async_remote_copy(
            src_ref=attn.at[token_rows(k)],
            dst_ref=heads.at[:, mine],
            send_sem=head_send.at[k - 1],
            recv_sem=head_recv.at[k - 1],
            device_id={"tp": peer[k]},
            device_id_type=MESH,
        )

    for k in far_first:
        attn[token_rows(k), :] = (acc[token_rows(k), :] / mass[token_rows(k), :]).astype(attn.dtype)
        head_copy(k).start()
    heads[:, mine] = (acc[token_rows(0), :] / mass[token_rows(0), :]).astype(heads.dtype)

    def head_arrival(k):
        cols = pl.ds(pl.multiple_of(peer[k] * width, width), width)
        return pltpu.make_async_remote_copy(
            src_ref=attn.at[token_rows(k)],
            dst_ref=heads.at[:, cols],
            send_sem=head_send.at[k - 1],
            recv_sem=head_recv.at[k - 1],
            device_id={"tp": peer[k]},
            device_id_type=MESH,
        )

    if half > 2:
        relay(UP, 2)
    for load in loads[4:]:
        load.wait()
    for k in range(1, tp):
        head_arrival(k).wait_recv()

    features = middle.shape[1]
    lanes = min(256, features)

    def feature_cols(c):
        return pl.ds(pl.multiple_of(c * lanes, lanes), lanes)

    def project(c, total):
        cols = feature_cols(c)
        made = rest[:, cols].astype(jnp.float32) + jnp.dot(
            heads[...], weight[:, cols], preferred_element_type=jnp.float32
        )
        middle[:, cols] = made
        return total + jnp.sum(made * made, axis=1, keepdims=True)

    squares = lax.fori_loop(0, features // lanes, project, jnp.zeros((own_rows, 1), jnp.float32))
    inverse = lax.rsqrt(squares / features + epsilon)

    def normalize(c, carry):
        cols = feature_cols(c)
        normed[pl.ds(0, own_rows), cols] = (middle[:, cols] * inverse * norm_gain[:, cols]).astype(normed.dtype)
        return carry

    lax.fori_loop(0, features // lanes, normalize, 0)

    def rows_of(k):
        return pl.ds(k * own_rows, own_rows)

    def norm_copy(k):
        source = 0 if k % 2 == 0 else k - 1
        return pltpu.make_async_remote_copy(
            src_ref=normed.at[rows_of(source)],
            dst_ref=normed.at[rows_of(k)],
            send_sem=norm_send.at[k - 1],
            recv_sem=norm_recv.at[k - 1],
            device_id={"tp": peer[k if k % 2 == 0 else 1]},
            device_id_type=MESH,
        )

    for k in range(2, tp, 2):
        norm_copy(k).start()
    norm_copy(1).start()
    for step in range(3, half):
        relay(UP, step)
    launch(DOWN)
    for k in range(2, tp, 2):
        norm_copy(k).wait_recv()
        norm_copy(k + 1).start()
    for k in range(1, tp, 2):
        norm_copy(k).wait_recv()
    relay(UP, half)

    blocks = [(me, None)]
    for step in range(1, half + 1):
        for way in (0, 1) if step < half else (0,):
            blocks.append((at_distance(step if way else -step), slot(way, step)))

    depth = up_own.shape[0]
    hidden = up_own.shape[1]
    all_rows = tp * own_rows
    row_tile = all_rows // 2
    hid_tile = min(256, hidden)
    act = weight.at[pl.ds(0, all_rows), pl.ds(0, hidden)]

    def units(i, carry):
        here = pl.ds(pl.multiple_of((i % 2) * row_tile, row_tile), row_tile)
        cols = pl.ds(pl.multiple_of((i // 2) * hid_tile, hid_tile), hid_tile)
        total = None
        for source, place in blocks:
            there = pl.ds(pl.multiple_of(source * depth, depth), depth)
            matrix = up_own[:, cols] if place is None else up_buf[place, :, cols]
            product = jnp.dot(normed[here, there], matrix, preferred_element_type=jnp.float32)
            total = product if total is None else total + product
        total = jnp.maximum(total, 0.0)
        act[here, cols] = (total * total).astype(act.dtype)
        return carry

    lax.fori_loop(0, 2 * (hidden // hid_tile), units, 0)

    out_cols = down_own.shape[1]

    def part_copy(c, k):
        return pltpu.make_async_remote_copy(
            src_ref=give.at[c, rows_of(k)],
            dst_ref=take.at[c, rows_of(k - 1)],
            send_sem=part_send.at[c, k - 1],
            recv_sem=part_recv.at[c, k - 1],
            device_id={"tp": peer[k]},
            device_id_type=MESH,
        )

    def contribute(c):
        source, place = blocks[c]
        matrix = down_own[...] if place is None else down_buf[place]
        for low in (row_tile, 0):
            here = pl.ds(low, row_tile)
            give[c, here, :] = jnp.dot(act[here, :], matrix, preferred_element_type=jnp.float32).astype(give.dtype)
            for k in range(1, tp):
                if low <= k * own_rows < low + row_tile:
                    part_copy(c, k).start()
        cols = pl.ds(pl.multiple_of(source * out_cols, out_cols), out_cols)
        middle[:, cols] += give[c, rows_of(0), :].astype(jnp.float32)

    def finish(c):
        source, place = blocks[c]
        cols = pl.ds(pl.multiple_of(source * out_cols, out_cols), out_cols)
        total = middle[:, cols]
        for k in range(1, tp):
            part_copy(c, k).wait_recv()
            total = total + take[c, rows_of(k - 1), :].astype(jnp.float32)
        out[:, cols] = total.astype(out.dtype)

    contribute(0)
    done = 0
    ready = 1
    for step in range(1, half + 1):
        relay(DOWN, step)
        fresh = 2 if step < half else 1
        for c in range(ready, ready + fresh):
            contribute(c)
        for c in range(done, ready):
            finish(c)
        done, ready = ready, ready + fresh
    for c in range(done, ready):
        finish(c)

    for kind in range(4):
        for step in range(1, half + 1):
            for part in (0, 1):
                for way in (0, 1):
                    if exists(way, step, part):
                        ring(kind, way, step, part).wait_send()
    for k in range(1, tp):
        head_copy(k).wait_send()
        norm_copy(k).wait_send()
        for c in range(count):
            part_copy(c, k).wait_send()


def local(
    order, tp, residual_in, queries, keys, values, query_gain, key_norm_gain, out_weight, norm_gain, up_weight, down_weight
):
    count = len(order)
    rows, width = queries.shape
    own_rows, features = residual_in.shape
    tables = rotary_tables(rows * count)
    anywhere = pl.BlockSpec(memory_space=pl.ANY)
    vmem = pl.BlockSpec(memory_space=pltpu.VMEM)
    bf16, f32 = jnp.bfloat16, jnp.float32
    others = lambda a: pltpu.VMEM((count - 1,) + a.shape, bf16)
    dma = pltpu.SemaphoreType.DMA
    return pl.pallas_call(
        functools.partial(layer_kernel, order, tp),
        out_shape=jax.ShapeDtypeStruct(residual_in.shape, bf16),
        in_specs=[anywhere] * 4 + [vmem] * 6 + [anywhere, vmem, anywhere, anywhere],
        out_specs=vmem,
        scratch_shapes=[
            pltpu.VMEM(keys.shape, bf16),
            pltpu.VMEM(keys.shape, bf16),
            pltpu.VMEM(values.shape, bf16),
            pltpu.VMEM(up_weight.shape, bf16),
            pltpu.VMEM(down_weight.shape, bf16),
            others(keys),
            others(values),
            others(up_weight),
            others(down_weight),
            pltpu.VMEM(queries.shape, bf16),
            pltpu.VMEM(queries.shape, bf16),
            pltpu.VMEM(queries.shape, f32),
            pltpu.VMEM(queries.shape, f32),
            pltpu.VMEM(queries.shape, f32),
            pltpu.VMEM((own_rows, width * tp), bf16),
            pltpu.VMEM(out_weight.shape, bf16),
            pltpu.VMEM(residual_in.shape, f32),
            pltpu.VMEM((tp * own_rows, features), bf16),
            pltpu.VMEM((count, tp * own_rows, down_weight.shape[1]), bf16),
            pltpu.VMEM((count, (tp - 1) * own_rows, down_weight.shape[1]), bf16),
            pltpu.VMEM(residual_in.shape, bf16),
            dma((7,)),
            dma((4, 2, count // 2, 2)),
            dma((4, 2, count // 2, 2)),
            dma((tp - 1,)),
            dma((tp - 1,)),
            dma((tp - 1,)),
            dma((tp - 1,)),
            dma((count, tp - 1)),
            dma((count, tp - 1)),
        ],
        compiler_params=pltpu.CompilerParams(
            collective_id=0, has_side_effects=True, vmem_limit_bytes=67043328
        ),
        name="layer",
    )(
        residual_in, queries, keys, values, query_gain[None], key_norm_gain[None], *tables,
        out_weight, norm_gain[None], up_weight, down_weight,
    )


def paired_kernel(
    depth, tp, residual, queries, keys, values, query_gain, key_gain, row_cos, row_sin, col_cos, col_sin,
    out_weight, norm_gain, up, down, out,
    key_raw, key_spare, key_all, value_all, query_raw, query_spare, query, attn, acc, best, mass, heads,
    weight, middle, normed, up_all, down_all, give, sibling, take, rest,
    load_sem, line_send, line_recv, swap_send, swap_recv, head_send, head_recv, norm_send, norm_recv,
    core_send, core_recv, part_send, part_recv, shown, out_sem,
):
    me = lax.axis_index("sp")
    rank = lax.axis_index("tp")
    layer = me // 2
    row = me % 2
    mate = me + 1 - 2 * row
    place = (me, mate)
    side = (row, 1 - row)
    peer = [rank] + [lookup([i ^ k for i in range(tp)], rank) for k in range(1, tp)]
    pairs = [(j, k) for k in range(tp) for j in (0, 1) if j or k]
    pairs.sort(key=lambda pair: (pair[1] < 2, -pair[0]))

    rows, own_width = queries.shape
    own_rows = heads.shape[0]
    wide = query.shape[1]
    group = wide // HEAD_WIDTH
    tile = min(256, rows)
    scale = HEAD_WIDTH ** (-0.5) * 1.4426950408889634
    hidden = up_all.shape[1]
    up_rows = up.shape[0]
    out_cols = down.shape[1]
    half_cols = out_cols // 2

    def block(index, size):
        return pl.ds(pl.multiple_of(index * size, size), size)

    loads = [
        pltpu.make_async_copy(src, dst, load_sem.at[i])
        for i, (src, dst) in enumerate((
            (values.at[:, block(row, HEAD_WIDTH)], value_all.at[me]),
            (keys, key_raw),
            (queries, query_raw),
            (up.at[:, block(row, hidden)], up_all.at[block(me, up_rows)]),
            (down.at[block(row, hidden)], down_all.at[me]),
            (residual, rest),
            (out_weight, weight),
        ))
    ]
    for load in loads:
        load.start()

    def inside(index):
        return (index >= 0) & (index < depth)

    barrier = pltpu.get_barrier_semaphore()
    for j, k in pairs:
        pl.semaphore_signal(barrier, inc=1, device_id={"sp": place[j], "tp": peer[k]}, device_id_type=MESH)
    for step in (-1, 1):

        @pl.when(inside(layer + step))
        def _():
            pl.semaphore_signal(barrier, inc=1, device_id={"sp": me + 2 * step}, device_id_type=MESH)

    ends = jnp.where(layer > 0, 1, 0) + jnp.where(layer < depth - 1, 1, 0)
    pl.semaphore_wait(barrier, len(pairs) + ends)

    def spot(kind, c):
        if kind == UP:
            return up_all.at[block(c, up_rows)]
        return {VALUE: value_all, KEY: key_all, DOWN: down_all}[kind].at[c]

    def pieces(kind, step, part):
        return (1, 2) if kind == DOWN and step == depth - 1 and part else (part,)

    def line(kind, way, step, part, sender):
        sign = 2 * way - 1
        split = kind == DOWN and step == depth - 1 and part
        line_row = min(part, 1) if kind == DOWN else side[part]
        there = spot(kind, (layer + sign * (step - 1 if sender else step)) * 2 + line_row)
        if split:
            there = there.at[:, pl.ds((part - 1) * half_cols, half_cols)]
        return pltpu.make_async_remote_copy(
            src_ref=there,
            dst_ref=there,
            send_sem=line_send.at[kind, way, step - 1, part],
            recv_sem=line_recv.at[kind, way, step - 1, part],
            device_id={"sp": me - 2 * sign},
            device_id_type=MESH,
        )

    def sends(way, step):
        sign = 2 * way - 1
        return inside(layer + sign * (step - 1)) & inside(layer - sign)

    def launch(kind, part):
        for way in (0, 1):

            @pl.when(sends(way, 1))
            def _():
                line(kind, way, 1, part, True).start()

    def relay(kind, step, part):
        for way in (0, 1):

            @pl.when(inside(layer + (2 * way - 1) * step))
            def _():
                line(kind, way, step, part, False).wait_recv()

            if step < depth - 1:

                @pl.when(sends(way, step + 1))
                def _():
                    for piece in pieces(kind, step + 1, part):
                        line(kind, way, step + 1, piece, True).start()

    QUERY = 4

    def swap(kind, sender):
        source = {
            VALUE: lambda: values.at[:, block(side[1], HEAD_WIDTH)],
            KEY: lambda: key_spare,
            UP: lambda: up.at[:, block(side[1], hidden)],
            DOWN: lambda: down.at[block(side[1], hidden)],
            QUERY: lambda: query_spare,
        }[kind]()
        turn = 0 if sender else 1
        there = query.at[block(side[turn], rows)] if kind == QUERY else spot(kind, place[turn])
        return pltpu.make_async_remote_copy(
            src_ref=source,
            dst_ref=there,
            send_sem=swap_send.at[kind],
            recv_sem=swap_recv.at[kind],
            device_id={"sp": mate},
            device_id_type=MESH,
        )

    def rotate(src, first_col, gain, dst, first_row, count):
        lane = lax.broadcasted_iota(jnp.int32, (GRID_W, HEAD_WIDTH), 1)
        even = (lane // (HEAD_WIDTH // 4)) % 2 == 0

        def body(r, carry):
            grid_row = me * (rows // GRID_W) + r
            cosine = col_cos[...] + row_cos[pl.ds(grid_row, 1), :]
            sine = col_sin[...] + row_sin[pl.ds(grid_row, 1), :]
            here = block(r, GRID_W)
            there = pl.ds(pl.multiple_of(first_row + r * GRID_W, GRID_W), GRID_W)
            for h in range(count):
                cols = pl.ds(pl.multiple_of(first_col + h * HEAD_WIDTH, HEAD_WIDTH), HEAD_WIDTH)
                v = src[here, cols].astype(jnp.float32)
                v = v * lax.rsqrt(jnp.mean(v * v, axis=-1, keepdims=True) + epsilon) * gain[...]
                turned = jnp.where(
                    even,
                    pltpu.roll(v, HEAD_WIDTH - HEAD_WIDTH // 4, 1),
                    pltpu.roll(v, HEAD_WIDTH // 4, 1),
                )
                dst[there, pl.ds(h * HEAD_WIDTH, HEAD_WIDTH)] = (v * cosine + turned * sine).astype(dst.dtype)
            return carry

        lax.fori_loop(0, rows // GRID_W, body, 0)

    def flash(c, first, base, length):
        columns = [pl.ds(g * HEAD_WIDTH, HEAD_WIDTH) for g in range(group)]

        def body(index, carry):
            key = key_all[c]
            value = value_all[c]
            value = jnp.concatenate([value, jnp.ones_like(value)], axis=1)
            chains = []
            for u in range(2):
                here = pl.ds(pl.multiple_of(base + (index * 2 + u) * tile, tile), tile)
                for cols in columns:
                    s = lax.dot_general(
                        query[here, cols], key, (((1,), (1,)), ((), ())), preferred_element_type=jnp.float32
                    )
                    chains.append((here, cols, s))
            for here, cols, s in chains:
                top = jnp.max(s, axis=1, keepdims=True) * scale
                if first:
                    newest = jnp.broadcast_to(top, (tile, HEAD_WIDTH))
                else:
                    old = best[here, cols]
                    newest = jnp.maximum(old, top)
                    factor = jnp.exp2(old - newest)
                p = jnp.exp2(s * scale - newest[:, :1])
                made = jnp.dot(p.astype(jnp.bfloat16), value, preferred_element_type=jnp.float32)
                part, total = made[:, :HEAD_WIDTH], made[:, HEAD_WIDTH:]
                best[here, cols] = newest
                if first:
                    mass[here, cols] = total
                    acc[here, cols] = part
                else:
                    mass[here, cols] = mass[here, cols] * factor + total
                    acc[here, cols] = acc[here, cols] * factor + part
            return carry

        lax.fori_loop(0, length // (tile * 2), body, 0)

    def each_way(step, line_row, work):
        def body(way, carry):
            index = layer + (2 * way - 1) * step

            @pl.when(inside(index))
            def _():
                work(index * 2 + line_row)

            return carry

        lax.fori_loop(0, 2, body, 0)

    def attend(step, part):
        each_way(step, side[part], lambda c: flash(c, False, 0, 2 * rows))

    def relay_pair(step, part):
        relay(VALUE, step, part)
        relay(KEY, step, part)

    swap(VALUE, True).start()
    loads[0].wait()
    launch(VALUE, 0)
    loads[1].wait()
    rotate(key_raw, row * HEAD_WIDTH, key_gain, key_all.at[me], 0, 1)
    launch(KEY, 0)
    rotate(key_raw, side[1] * HEAD_WIDTH, key_gain, key_spare, 0, 1)
    swap(KEY, True).start()
    swap(VALUE, False).wait_recv()
    launch(VALUE, 1)
    loads[2].wait()
    rotate(query_raw, side[1] * wide, query_gain, query_spare, 0, group)
    swap(QUERY, True).start()
    swap(KEY, False).wait_recv()
    launch(KEY, 1)
    swap(UP, True).start()
    loads[3].wait()
    launch(UP, 0)
    rotate(query_raw, row * wide, query_gain, query, row * rows, group)
    flash(me, True, row * rows, rows)
    relay_pair(1, 0)
    flash(mate, False, row * rows, rows)
    swap(QUERY, False).wait_recv()
    flash(me, True, side[1] * rows, rows)
    flash(mate, False, side[1] * rows, rows)
    events = [(step, part) for step in range(1, depth) for part in (0, 1)]
    swap_started = False
    for i, (step, part) in enumerate(events):
        later = events[i + 1] if i + 1 < len(events) else None
        if i and step == depth - 1:
            relay_pair(step, part)
        if later is not None and later[0] < depth - 1:
            relay_pair(*later)
        if (later is None or later[0] == depth - 1) and not swap_started:
            swap_started = True
            swap(UP, False).wait_recv()
            launch(UP, 1)
            relay(UP, 1, 0)
            swap(DOWN, True).start()
        attend(step, part)

    width = own_width

    def token_rows(j, k):
        return block(side[j] * tp + peer[k], own_rows)

    def head_copy(j, k, sender):
        at = (row, rank) if sender else (side[j], peer[k])
        cols = pl.ds(pl.multiple_of(at[1] * width + at[0] * wide, wide), wide)
        index = j * tp + k - 1
        return pltpu.make_async_remote_copy(
            src_ref=attn.at[token_rows(j, k)],
            dst_ref=heads.at[:, cols],
            send_sem=head_send.at[index],
            recv_sem=head_recv.at[index],
            device_id={"sp": place[j], "tp": peer[k]},
            device_id_type=MESH,
        )

    for j, k in pairs:
        here = token_rows(j, k)
        attn[here, :] = (acc[here, :] / mass[here, :]).astype(attn.dtype)
        head_copy(j, k, True).start()
    here = token_rows(0, 0)
    heads[:, pl.ds(pl.multiple_of(rank * width + row * wide, wide), wide)] = (acc[here, :] / mass[here, :]).astype(heads.dtype)
    relay(UP, 1, 1)
    for load in loads[4:]:
        load.wait()
    for j, k in pairs:
        head_copy(j, k, False).wait_recv()

    features = middle.shape[1]
    lanes = min(256, features)

    def project(c, total):
        cols = block(c, lanes)
        made = rest[:, cols].astype(jnp.float32) + jnp.dot(
            heads[...], weight[:, cols], preferred_element_type=jnp.float32
        )
        middle[:, cols] = made
        return total + jnp.sum(made * made, axis=1, keepdims=True)

    squares = lax.fori_loop(0, features // lanes, project, jnp.zeros((own_rows, 1), jnp.float32))
    inverse = lax.rsqrt(squares / features + epsilon)

    def normalize(c, carry):
        cols = block(c, lanes)
        normed[pl.ds(0, own_rows), cols] = (middle[:, cols] * inverse * norm_gain[:, cols]).astype(normed.dtype)
        return carry

    lax.fori_loop(0, features // lanes, normalize, 0)

    def rows_of(j, k):
        return pl.ds((j * tp + k) * own_rows, own_rows)

    half_own = own_rows // 2

    def norm_copy(j, k, h):
        size = own_rows if k % 2 else half_own
        if k % 2:
            source, target = (j, k - 1), (0, 1)
        elif j and k:
            source, target = ((1, 0), (0, k)) if h else ((0, k), (1, 0))
        else:
            source, target = (0, 0), (j, k)
        index = j * tp + k - 1
        return pltpu.make_async_remote_copy(
            src_ref=normed.at[pl.ds((source[0] * tp + source[1]) * own_rows + h * half_own, size)],
            dst_ref=normed.at[pl.ds((j * tp + k) * own_rows + h * half_own, size)],
            send_sem=norm_send.at[index, h],
            recv_sem=norm_recv.at[index, h],
            device_id={"sp": place[target[0]], "tp": peer[target[1]]},
            device_id_type=MESH,
        )

    def norm_halves(k):
        return (0,) if k % 2 else (0, 1)

    for h in (0, 1):
        for k in range(2, tp, 2):
            norm_copy(0, k, h).start()
        norm_copy(1, 0, 1 - h).start()
    norm_copy(0, 1, 0).start()
    for step in range(2, depth - 1):
        for part in (0, 1):
            relay(UP, step, part)
    swap(DOWN, False).wait_recv()
    launch(DOWN, 0)
    launch(DOWN, 1)
    for k in range(2, tp, 2):
        norm_copy(0, k, 0).wait_recv()
        norm_copy(1, k, 0).start()
    norm_copy(1, 0, 1).wait_recv()
    for k in range(2, tp, 2):
        norm_copy(1, k, 1).start()
    for k in range(2, tp, 2):
        norm_copy(0, k, 1).wait_recv()
        norm_copy(0, k + 1, 0).start()
    norm_copy(1, 0, 0).wait_recv()
    norm_copy(1, 1, 0).start()
    for part in (0, 1):
        relay(UP, depth - 1, part)
    for k in range(1, tp, 2):
        norm_copy(0, k, 0).wait_recv()

    all_rows = 2 * tp * own_rows
    row_tile = min(512, tp * own_rows)
    hid_tile = min(256, hidden)
    act = weight.at[pl.ds(0, all_rows), pl.ds(0, hidden)]

    def units(j):
        tiles = tp * own_rows // row_tile

        def body(i, carry):
            here = pl.ds(pl.multiple_of(j * tp * own_rows + (i % tiles) * row_tile, row_tile), row_tile)
            cols = block(i // tiles, hid_tile)
            total = jnp.dot(normed[here, :], up_all[:, cols], preferred_element_type=jnp.float32)
            total = jnp.maximum(total, 0.0)
            act[here, cols] = (total * total).astype(act.dtype)
            return carry

        lax.fori_loop(0, tiles * (hidden // hid_tile), body, 0)

    units(0)
    for k in range(2, tp, 2):
        for h in (0, 1):
            norm_copy(1, k, h).wait_recv()
        norm_copy(1, k + 1, 0).start()
    for k in range(1, tp, 2):
        norm_copy(1, k, 0).wait_recv()
    units(1)

    far = [(j, k) for j, k in pairs if k % 2 == 0]

    pair_rows = 2 * own_rows

    def columns_of(h):
        return pl.ds(h * half_cols, half_cols)

    def core_copy(c, t, h):
        return pltpu.make_async_remote_copy(
            src_ref=give.at[c, pl.ds(pl.multiple_of(t * pair_rows + own_rows, own_rows), own_rows), columns_of(h)],
            dst_ref=sibling.at[c, block(t, own_rows), columns_of(h)],
            send_sem=core_send.at[c, t, h],
            recv_sem=core_recv.at[c, t, h],
            device_id={"tp": peer[1]},
            device_id_type=MESH,
        )

    def part_copy(c, j, k, h):
        index = far.index((j, k))
        return pltpu.make_async_remote_copy(
            src_ref=give.at[c, rows_of(j, k), columns_of(h)],
            dst_ref=take.at[c, pl.ds(index * own_rows, own_rows), columns_of(h)],
            send_sem=part_send.at[c, index, h],
            recv_sem=part_recv.at[c, index, h],
            device_id={"sp": place[j], "tp": peer[k]},
            device_id_type=MESH,
        )

    def contribute(c, halves=(0, 1)):
        span = pl.ds(halves[0] * half_cols, len(halves) * half_cols)

        def body(i, carry):
            t = tp - 1 - i
            here = block(t, pair_rows)
            give[c, here, span] = jnp.dot(
                act[here, :], down_all[c, :, span], preferred_element_type=jnp.float32
            ).astype(give.dtype)
            for h in halves:
                core_copy(c, t, h).start()
            return carry

        lax.fori_loop(0, tp, body, 0)

        def both(j, k, h):
            t = j * (tp // 2) + k // 2
            core_copy(c, t, h).wait_recv()
            mine = give[c, rows_of(j, k), columns_of(h)].astype(jnp.float32)
            return mine + sibling[c, pl.ds(t * own_rows, own_rows), columns_of(h)].astype(jnp.float32)

        for j, k in far:
            for h in halves:
                give[c, rows_of(j, k), columns_of(h)] = both(j, k, h).astype(give.dtype)
                part_copy(c, j, k, h).start()
        for h in halves:
            cols = pl.ds(pl.multiple_of(c * out_cols + h * half_cols, half_cols), half_cols)
            middle[:, cols] += both(0, 0, h)

    def out_copy(c):
        cols = block(c, out_cols)
        return pltpu.make_async_copy(shown.at[:, cols], out.at[:, cols], out_sem.at[c])

    def finish(c, halves=(0, 1)):
        for h in halves:
            cols = pl.ds(pl.multiple_of(c * out_cols + h * half_cols, half_cols), half_cols)
            total = middle[:, cols]
            for index, (j, k) in enumerate(far):
                part_copy(c, j, k, h).wait_recv()
                total = total + take[c, pl.ds(index * own_rows, own_rows), columns_of(h)].astype(jnp.float32)
            shown[:, cols] = total.astype(shown.dtype)
        out_copy(c).start()

    def line_done(kind, steps):
        for step in steps:
            for part in (0,) + pieces(kind, step, 1):
                for way in (0, 1):

                    @pl.when(sends(way, step))
                    def _():
                        line(kind, way, step, part, True).wait_send()

    def drain(c):
        for h in (0, 1):
            for t in range(tp):
                core_copy(c, t, h).wait_send()
            for j, k in far:
                part_copy(c, j, k, h).wait_send()

    def settle(c):
        finish(c)
        drain(c)

    steps = range(1, depth)
    relay(DOWN, 1, 0)
    for part in (0, 1):
        contribute(layer * 2 + part)
    for i, (step, part) in enumerate(events):
        if step == depth - 1:
            if not part:
                for kind in (VALUE, KEY, UP):
                    line_done(kind, steps)
                for kind in range(5):
                    swap(kind, True).wait_send()
                for j, k in pairs:
                    head_copy(j, k, True).wait_send()
                    for h in norm_halves(k):
                        norm_copy(j, k, h).wait_send()
            else:
                for r in (0, 1):
                    settle(layer * 2 + r)
                for event in events[:-4]:
                    each_way(*event, settle)
        if i:
            relay(DOWN, step, part)
        if step == depth - 1 and part:
            each_way(step, part, functools.partial(contribute, halves=(0,)))
            line_done(DOWN, steps[:-1])
            each_way(*events[-4], settle)
            relay(DOWN, step, 2)
            each_way(step, part, functools.partial(contribute, halves=(1,)))
        else:
            each_way(step, part, contribute)
    for event in events[-3:]:
        each_way(*event, settle)
    line_done(DOWN, steps[-1:])

    def written(c, carry):
        out_copy(c).wait()
        return carry

    lax.fori_loop(0, 2 * depth, written, 0)


def paired_local(
    depth, tp, residual_in, queries, keys, values, query_gain, key_norm_gain, out_weight, norm_gain, up_weight, down_weight
):
    count = 2 * depth
    rows, width = queries.shape
    own_rows, features = residual_in.shape
    tables = rotary_tables(rows * count)
    anywhere = pl.BlockSpec(memory_space=pl.ANY)
    vmem = pl.BlockSpec(memory_space=pltpu.VMEM)
    bf16, f32 = jnp.bfloat16, jnp.float32
    dma = pltpu.SemaphoreType.DMA
    wide = width // 2
    hidden = up_weight.shape[1] // 2
    out_cols = down_weight.shape[1]
    group_rows = 2 * tp * own_rows
    far = tp - 1
    made = pl.pallas_call(
        functools.partial(paired_kernel, depth, tp),
        out_shape=jax.ShapeDtypeStruct(residual_in.shape, bf16),
        in_specs=[anywhere] * 4 + [vmem] * 6 + [anywhere, vmem, anywhere, anywhere],
        out_specs=anywhere,
        scratch_shapes=[
            pltpu.VMEM(keys.shape, bf16),
            pltpu.VMEM((rows, HEAD_WIDTH), bf16),
            pltpu.VMEM((count, rows, HEAD_WIDTH), bf16),
            pltpu.VMEM((count, rows, HEAD_WIDTH), bf16),
            pltpu.VMEM(queries.shape, bf16),
            pltpu.VMEM((rows, wide), bf16),
            pltpu.VMEM((2 * rows, wide), bf16),
            pltpu.VMEM((2 * rows, wide), bf16),
            pltpu.VMEM((2 * rows, wide), f32),
            pltpu.VMEM((2 * rows, wide), f32),
            pltpu.VMEM((2 * rows, wide), f32),
            pltpu.VMEM((own_rows, width * tp), bf16),
            pltpu.VMEM(out_weight.shape, bf16),
            pltpu.VMEM(residual_in.shape, f32),
            pltpu.VMEM((group_rows, features), bf16),
            pltpu.VMEM((features, hidden), bf16),
            pltpu.VMEM((count, hidden, out_cols), bf16),
            pltpu.VMEM((count, group_rows, out_cols), bf16),
            pltpu.VMEM((count, group_rows // 2, out_cols), bf16),
            pltpu.VMEM((count, far * own_rows, out_cols), bf16),
            pltpu.VMEM(residual_in.shape, bf16),
            dma((7,)),
            dma((4, 2, depth - 1, 3)),
            dma((4, 2, depth - 1, 3)),
            dma((5,)),
            dma((5,)),
            dma((2 * tp - 1,)),
            dma((2 * tp - 1,)),
            dma((2 * tp - 1, 2)),
            dma((2 * tp - 1, 2)),
            dma((count, tp, 2)),
            dma((count, tp, 2)),
            dma((count, far, 2)),
            dma((count, far, 2)),
            pltpu.VMEM(residual_in.shape, bf16),
            dma((count,)),
        ],
        compiler_params=pltpu.CompilerParams(
            collective_id=0, has_side_effects=True, vmem_limit_bytes=67043328
        ),
        name="layer",
    )(
        residual_in, queries, keys, values, query_gain[None], key_norm_gain[None], *tables,
        out_weight, norm_gain[None], up_weight, down_weight,
    )
    return pl.pallas_call(
        hand_over,
        out_shape=jax.ShapeDtypeStruct(made.shape, bf16),
        in_specs=[anywhere],
        out_specs=anywhere,
        scratch_shapes=[pltpu.VMEM(made.shape, bf16), dma((2, 4))],
        name="hand_over",
    )(made)


def hand_over(made, out, held, sem):
    size = made.shape[0] // 4
    spans = [pl.ds(i * size, size) for i in range(4)]
    taken = [pltpu.make_async_copy(made.at[span], held.at[span], sem.at[0, i]) for i, span in enumerate(spans)]
    given = [pltpu.make_async_copy(held.at[span], out.at[span], sem.at[1, i]) for i, span in enumerate(spans)]
    for copy in taken:
        copy.start()
    for take, give in zip(taken, given):
        take.wait()
        give.start()
    for copy in given:
        copy.wait()


def solution(mesh):
    order = ring_order(mesh)
    count, tp = mesh.shape["sp"], mesh.shape["tp"]

    def step(*arrays):
        kv_heads = arrays[2].shape[1] // HEAD_WIDTH
        if plane_width(mesh) == 2 and count >= 6 and tp % 2 == 0 and kv_heads == 2:
            return paired_local(count // 2, tp, *arrays)
        return local(order, tp, *arrays)

    return jax.shard_map(
        step,
        mesh=mesh,
        in_specs=(
            P(("sp", "tp"), None),
            P("sp", "tp"),
            P("sp", "tp"),
            P("sp", "tp"),
            P(),
            P(),
            P(),
            P(),
            P("sp", "tp"),
            P("tp", "sp"),
        ),
        out_specs=P(("sp", "tp"), None),
        check_vma=False,
    )
```
